32 devices in a mesh: grp: 2 (over y), ep: 8 (over z, x), tp: 2 (over core).
Axes of the slice: x: 2, y: 2, z: 4, core: 2. Of those that a mesh axis runs over, the one named last changes fastest.
Arguments:
- tokens: bfloat16 [4096, 2048], P(('grp', 'ep', 'tp')), parts along dimension 0, may hold values from -6 to 6
- norm_gain: float32 [2048], replicated, may hold values from 0.1 to 1.9
- expert_ids: int32 [4096, 2], P(('grp', 'ep', 'tp')), parts along dimension 0, may hold values from 0 to 3, all different within a row; in each aligned block of 128 rows (0 to 127, 128 to 255, ...) at most 80 rows name the same one
- route_weights: float32 [4096, 2], P(('grp', 'ep', 'tp')), parts along dimension 0, may hold values from 0.1 to 0.9
- w_gate: bfloat16 [2048, 14336], P(None, ('ep', 'tp')), may hold values from -0.125 to 0.125
- w_up: bfloat16 [2048, 14336], P(None, ('ep', 'tp')), may hold values from -0.125 to 0.125
- w_down: bfloat16 [14336, 2048], P(('ep', 'tp')), may hold values from -0.09375 to 0.09375
Outputs:
- mixed_out: bfloat16 [4096, 2048], P(('grp', 'ep', 'tp')), parts along dimension 0
The draws below stay inside these ranges and needn't reach their ends.
There are 2 independent parts, one for each index of `grp`. The reference program is written for one: setup_inputs(seed, part) draws one part's arguments, and reference() takes and returns one part's arrays. A program takes and returns all parts, laid end to end along the dimension named above; an argument that names none is the same for every part. Nothing has to cross between parts.
Inputs may be any that keep to these rules, and one draw needn't show every extreme that they name: `expert_ids`: each row names 2 different experts. Among the rows of one device no expert is named more than 80 times, and in every draw some expert is named exactly 80 times by one device's rows.
All inputs are finite; a program needn't handle non-finite values.
Results may differ from the reference program's by a relative error of at most 0.01.
Values may be sent and summed in bfloat16 or wider, within the bound.
A program may use at most 128 MiB of HBM per device.

```python
import math
import jax
import jax.numpy as jnp
import numpy as np
from jax import lax

D = 2048
FF = 3584
TOP_K = 2
TOK_DEV = 128
EXPERTS = 4
CAP = 80
TOKENS = 2048
N_TP = 2


def level_of(stream_key, extent, pieces, low, largest):
    loudness = 1.0
    for dim, blocks in pieces:
        heights = jax.random.uniform(jax.random.fold_in(jax.random.fold_in(stream_key, 6), dim), (blocks,), jnp.float32, low / len(pieces), largest / len(pieces))
        loudness = loudness * jnp.repeat(jnp.exp(heights), extent[dim] // blocks).reshape((-1,) + (1,) * (len(extent) - 1 - dim))
    return loudness


def routed_block(stream_key, own, number, rows, amount, top, reach, slope):
    order = jax.random.permutation(stream_key, amount)
    heavy_load, common = shares(amount, rows * top, reach, slope, True), shares(amount, rows * top, reach, slope, False)
    places = jnp.arange(amount)

    def named(tallies, turn):
        used = int((tallies > 0).sum())
        fixed = max(1, used // 4)
        passed = fixed + (places - fixed + turn * (used - fixed)) % max(1, amount - fixed)
        return jnp.zeros((amount,), jnp.int32).at[order[jnp.where(places < fixed, places, passed)]].set(jnp.asarray(tallies, jnp.int32))

    tallies = jnp.where(number % 4 == 0, named(heavy_load, number // 4), named(common, number - number // 4 - 1))
    mixed = jax.random.permutation(jax.random.fold_in(own, 3), amount)
    donor, taker = mixed[0:amount // 2 * 2:2], mixed[1:amount // 2 * 2:2]
    margin = jnp.minimum(tallies[donor] - 1, reach - tallies[taker]) // 2
    margin = jnp.where((donor == order[0]) | (taker == order[0]) | (tallies[taker] == 0), 0, jnp.maximum(margin, 0))
    passed = jax.random.randint(jax.random.fold_in(own, 4), (amount // 2,), 0, 1 << 20) % (margin + 1)
    tallies = tallies.at[donor].add(-passed).at[taker].add(passed)
    members = jnp.searchsorted(jnp.cumsum(tallies), jnp.arange(rows * top), side="right").astype(jnp.int32)
    table = members.reshape(top, rows).T
    table = table[jax.random.permutation(jax.random.fold_in(own, 1), rows)]
    turn = jax.random.randint(jax.random.fold_in(own, 2), (rows, 1), 0, top)
    return jnp.take_along_axis(table, (jnp.arange(top)[None, :] + turn) % top, axis=1)


def shares(count, total, reach, lean, full):
    portions = [(1 << 20) // math.isqrt(rank ** lean) + 1 for rank in range(1, count + 1)]
    largest = reach if full else min(reach, max(-(-total // count), total * portions[0] // sum(portions)))
    least = 1 if total - largest >= count - 1 else 0
    given, surplus = [largest] + [least] * (count - 1), total - largest - least * (count - 1)
    while surplus > 0:
        free = [i for i in range(1, count) if given[i] < largest] or [i for i in range(1, count) if given[i] < reach]
        whole, budget = sum([portions[i] for i in free]), surplus
        for i in free:
            addition = min(reach - given[i], max(1, budget * portions[i] // whole), surplus)
            given[i] = given[i] + addition
            surplus = surplus - addition
    return np.array(given)


def noise(rng, shape, scale, reach, shards=(), kind=jnp.bfloat16):
    drawn = jax.random.normal(rng, shape, jnp.float32) * scale
    if len(shards) > 0:
        drawn = level_of(rng, shape, shards, -0.22, 0.18) * drawn
    return jnp.clip(drawn, min=-reach, max=reach).astype(kind)


def setup_inputs(seed: int = 0, part: int = 0) -> dict:
    arg_keys = jax.random.split(jax.random.key(seed), 8)
    part_splits = jax.random.split(jax.random.fold_in(arg_keys[7], part), 8)
    tokens = noise(part_splits[0], (TOKENS, D), 1.0, 6.0, ((0, 16),))
    norm_gain = jnp.clip(1.0 + 0.18 * jax.random.normal(arg_keys[1], (D,), jnp.float32), 0.1, 1.9)
    expert_ids_keys = jax.random.split(jax.random.fold_in(part_splits[2], 1), TOKENS // TOK_DEV)
    expert_ids_turns = jax.random.permutation(jax.random.fold_in(part_splits[2], 3), TOKENS // TOK_DEV)
    expert_ids = jax.vmap(lambda own, number: routed_block(jax.random.fold_in(part_splits[2], 2), own, number, TOK_DEV, EXPERTS, TOP_K, CAP, 2))(expert_ids_keys, expert_ids_turns).reshape((TOKENS, TOP_K))
    route_weights = jnp.clip(0.1 + 0.79999997 * jax.random.uniform(part_splits[3], (TOKENS, TOP_K), jnp.float32) ** level_of(part_splits[3], (TOKENS, TOP_K), ((0, 16),), -0.2, 0.2), 0.1, 0.9)
    w_gate = noise(arg_keys[4], (D, EXPERTS * FF), D ** -0.5, 0.125, ((1, 16),))
    w_up = noise(arg_keys[5], (D, EXPERTS * FF), D ** -0.5, 0.125, ((1, 16),))
    w_down = noise(arg_keys[6], (EXPERTS * FF, D), FF ** -0.5, 0.09375, ((0, 16),))
    return dict(tokens=tokens, norm_gain=norm_gain, expert_ids=expert_ids, route_weights=route_weights, w_gate=w_gate, w_up=w_up, w_down=w_down)


def reference(tokens, norm_gain, expert_ids, route_weights, w_gate, w_up, w_down):
    values = tokens.astype(jnp.float32)
    scale_rows = lax.rsqrt(lax.optimization_barrier(jnp.mean(values * values, axis=1, keepdims=True)) + 1e-06)
    normed = (values * scale_rows * norm_gain).astype(jnp.bfloat16)
    token_total = tokens.shape[0]
    sources = token_total // TOK_DEV
    per_source = expert_ids.reshape(sources, TOK_DEV * TOP_K)
    onehot = (per_source[:, :, None] == jnp.arange(EXPERTS, dtype=jnp.int32)[None, None, :]).astype(jnp.int32)
    earlier = jnp.cumsum(onehot, axis=1) - onehot
    slot_base = lax.optimization_barrier(jnp.sum(earlier * onehot, axis=2)).reshape(-1).astype(jnp.int32)
    flat_ids = expert_ids.reshape(-1).astype(jnp.int32)
    token_index = (jnp.arange(flat_ids.shape[0], dtype=jnp.int32) // TOP_K).astype(jnp.int32)
    source_index = (token_index // TOK_DEV).astype(jnp.int32)
    slot_index = jnp.remainder(slot_base + source_index, CAP).astype(jnp.int32)
    position = ((flat_ids * sources + source_index) * CAP + slot_index).astype(jnp.int32)
    slot_table = jnp.full((EXPERTS * sources * CAP,), token_total, jnp.int32).at[position].set(token_index)
    slot_table = slot_table.reshape(EXPERTS, sources * CAP)
    padded = jnp.concatenate([normed, jnp.zeros((1, normed.shape[1]), jnp.bfloat16)], axis=0)
    piece_width = FF // (2 * N_TP)

    def one_expert(inputs):
        expert, rows_index = inputs
        in_rows = padded[rows_index]
        first_col = (expert * FF).astype(jnp.int32)
        gate_part = jnp.dot(in_rows, lax.dynamic_slice_in_dim(w_gate, first_col, FF, 1), preferred_element_type=jnp.float32)
        up_part = jnp.dot(in_rows, lax.dynamic_slice_in_dim(w_up, first_col, FF, 1), preferred_element_type=jnp.float32)
        hidden = (jax.nn.silu(gate_part) * up_part).astype(jnp.bfloat16)
        down_rows = lax.dynamic_slice_in_dim(w_down, first_col, FF, 0)
        expert_total = jnp.zeros((in_rows.shape[0], normed.shape[1]), jnp.float32)
        for half_index in range(2):
            half_sum = jnp.zeros((in_rows.shape[0], normed.shape[1]), jnp.float32)
            for core_index in range(N_TP):
                begin = (half_index * N_TP + core_index) * piece_width
                partial_value = jnp.dot(hidden[:, begin:begin + piece_width], down_rows[begin:begin + piece_width], preferred_element_type=jnp.float32)
                half_sum = half_sum + lax.optimization_barrier(partial_value.astype(jnp.bfloat16)).astype(jnp.float32)
            expert_total = expert_total + lax.optimization_barrier(half_sum.astype(jnp.bfloat16)).astype(jnp.float32)
        return lax.optimization_barrier(expert_total.astype(jnp.bfloat16)).astype(jnp.float32)
    results = lax.map(one_expert, (jnp.arange(EXPERTS, dtype=jnp.int32), slot_table))
    picked = results.reshape(-1, normed.shape[1])[position].reshape(token_total, TOP_K, normed.shape[1])
    return lax.optimization_barrier(jnp.sum(picked * route_weights[:, :, None], axis=1)).astype(jnp.bfloat16)
```

```python
import functools

import jax
import jax.numpy as jnp
from jax import lax
from jax.experimental import pallas as pl
from jax.experimental.pallas import tpu as pltpu
from jax.sharding import PartitionSpec as P

MESH = pl.DeviceIdType.MESH
LANE = 128
PIECES = 2
STAGES = 0
SCHEDULE = (
    ("near", 0, 0, 0),
    ("spread", -1, 1, 0),
    ("pass_on", 0, 0, 0),
    ("far", 0, 0, 0),
    ("give", 0, 1, 0),
    ("finish", 1, 1, -1),
)


def mix_index(first, second, count):
    total = first * 0
    bit = 1
    while bit < count:
        one, two = (first // bit) % 2, (second // bit) % 2
        total = total + bit * (one + two - 2 * one * two)
        bit *= 2
    return total


def kernel(
    experts, cap,
    tok_hbm, gain_hbm, ids_hbm, weight_hbm, gate_ref, up_ref, down_ref,
    out_ref,
    tok_ref, gain_ref, ids_ref, weight_ref, norm, names, ranks, mixing, xs, xa, hid, po, rd, cx, rx, fo, ret, wgu, wd,
    in_sem, gate_sem, up_sem, down_sem,
    z_send, z_recv, x_send, x_recv, d_send, d_recv, e_send, e_recv,
    r_send, r_recv, v_send, v_recv, w_send, w_recv,
):
    ep, c = lax.axis_index("ep"), lax.axis_index("tp")
    p, h = ep // 2, ep % 2
    toks, width = tok_ref.shape
    tiles = wgu.shape[0]
    part_width = width // PIECES
    across = {"ep": 2 * p + 1 - h, "tp": c}
    beside = {"ep": ep, "tp": 1 - c}

    def plane(q):
        return {"ep": 2 * q + h, "tp": c}

    loads = [
        pltpu.make_async_copy(src, dst, in_sem.at[n]) for n, (src, dst) in enumerate((
            (tok_hbm, tok_ref), (gain_hbm, gain_ref), (ids_hbm, ids_ref), (weight_hbm, weight_ref)))]
    for load in loads:
        load.start()

    barrier = pltpu.get_barrier_semaphore()

    def greet(k, carry):
        pl.semaphore_signal(barrier, inc=1, device_id=plane(mix_index(p, k, experts)), device_id_type=MESH)
        return carry

    lax.fori_loop(1, experts, greet, 0)
    pl.semaphore_signal(barrier, inc=1, device_id=across, device_id_type=MESH)
    pl.semaphore_signal(barrier, inc=1, device_id=beside, device_id_type=MESH)

    def gate_copy(j):
        return pltpu.make_async_copy(
            gate_ref.at[:, pl.ds(j * LANE, LANE)], wgu.at[j, :, pl.ds(0, LANE)], gate_sem.at[j])

    def up_copy(j):
        return pltpu.make_async_copy(
            up_ref.at[:, pl.ds(j * LANE, LANE)], wgu.at[j, :, pl.ds(LANE, LANE)], up_sem.at[j])

    down_copy = pltpu.make_async_copy(down_ref, wd, down_sem)
    for j in range(tiles):
        gate_copy(j).start()
        up_copy(j).start()
    down_copy.start()

    row = lax.broadcasted_iota(jnp.int32, (toks, toks), 0)
    col = lax.broadcasted_iota(jnp.int32, (toks, toks), 1)
    before = (row < col).astype(jnp.float32).astype(jnp.bfloat16)
    slots = lax.broadcasted_iota(jnp.int32, (cap, toks), 0).astype(jnp.float32)
    for load in loads[1:]:
        load.wait()
    kinds = lax.broadcasted_iota(jnp.int32, names.shape, 0)
    names[...] = ((ids_ref[0:1, :] == kinds) | (ids_ref[1:2, :] == kinds)).astype(jnp.float32)
    ranks[...] = jnp.dot(names[...].astype(jnp.bfloat16), before, preferred_element_type=jnp.float32)

    loads[0].wait()
    values = tok_ref[...].astype(jnp.float32)
    scale_rows = lax.rsqrt(jnp.mean(values * values, axis=1, keepdims=True) + 1e-06)
    norm[...] = (values * scale_rows * gain_ref[...]).astype(jnp.bfloat16)

    def remote(src, dst, send, recv, target):
        return pltpu.make_async_remote_copy(
            src_ref=src, dst_ref=dst, send_sem=send, recv_sem=recv, device_id=target, device_id_type=MESH)

    def cut(ref, index, g):
        return ref.at[index, :, pl.ds(g * part_width, part_width)]

    def z_pair(k, g, origin):
        q = mix_index(p, k, experts)
        n = PIECES * k + g
        return remote(
            cut(xs, q, g), cut(xa, 4 * origin(q) + 2 * h + c, g), z_send.at[n], z_recv.at[n], plane(q))

    def z_copy(k, g):
        return z_pair(k, g, lambda q: p)

    def z_land(k, g):
        return z_pair(k, g, lambda q: q)

    def mine(k, half, core, g):
        return cut(xa, 4 * mix_index(p, k, experts) + 2 * half + core, g)

    def shift(k, g, there, here, send, recv, target):
        n = PIECES * k + g
        return remote(mine(k, *there, g), mine(k, *here, g), send.at[n], recv.at[n], target)

    def x_copy(k, g):
        return shift(k, g, (h, c), (h, c), x_send, x_recv, across)

    def x_land(k, g):
        return shift(k, g, (h, c), (1 - h, c), x_send, x_recv, across)

    def d_copy(k, g):
        return shift(k, g, (h, c), (h, c), d_send, d_recv, beside)

    def d_land(k, g):
        return shift(k, g, (h, c), (h, 1 - c), d_send, d_recv, beside)

    def e_copy(k, g):
        return shift(k, g, (1 - h, c), (1 - h, c), e_send, e_recv, beside)

    def e_land(k, g):
        return shift(k, g, (1 - h, c), (1 - h, 1 - c), e_send, e_recv, beside)

    def r_copy(k, half, g):
        n = 2 * (PIECES * k + g) + half
        return remote(
            cut(po, 4 * k + 2 * half + 1 - c, g), cut(rd, 2 * k + half, g),
            r_send.at[n], r_recv.at[n], beside)

    def v_copy(k, g):
        n = PIECES * k + g
        return remote(cut(cx, 2 * k + 1 - h, g), cut(rx, k, g), v_send.at[n], v_recv.at[n], across)

    def w_pair(k, g, origin):
        q = mix_index(p, k, experts)
        n = PIECES * k + g
        return remote(cut(fo, k, g), cut(ret, origin(q), g), w_send.at[n], w_recv.at[n], plane(q))

    def w_copy(k, g):
        return w_pair(k, g, lambda q: p)

    def w_land(k, g):
        return w_pair(k, g, lambda q: q)

    def picked(e):
        spot = pl.ds(e, 1)
        pick = jnp.where(slots == ranks[spot, :], names[spot, :], 0.0).astype(jnp.bfloat16)
        return jnp.dot(pick, norm[...], preferred_element_type=jnp.float32).astype(jnp.bfloat16)

    pl.semaphore_wait(barrier, experts + 1)

    xa[4 * p + 2 * h + c] = picked(p)
    for g in range(PIECES):
        x_copy(0, g).start()
        d_copy(0, g).start()

    def fill(k, carry):
        e = mix_index(p, k, experts)
        xs[e] = picked(e)
        for g in range(PIECES):
            z_copy(k, g).start()
        return carry

    lax.fori_loop(1, experts, fill, 0)

    step = 2 * LANE

    def compute(k, half):
        rows = xa[pl.ds(4 * mix_index(p, k, experts) + 2 * half, 2)].reshape(2 * cap, width)
        for j in range(tiles):
            both = jnp.dot(rows, wgu[j], preferred_element_type=jnp.float32)
            gate, up = both[:, :LANE], both[:, LANE:]
            hid[:, j * LANE:(j + 1) * LANE] = (gate / (1.0 + jnp.exp(-gate)) * up).astype(jnp.bfloat16)
        many = part_width // step
        for g in range(PIECES):
            for n in range(g * many, (g + 1) * many):
                part = jnp.dot(hid[...], wd[:, n * step:(n + 1) * step], preferred_element_type=jnp.float32)
                po[pl.ds(4 * k + 2 * half, 2), :, n * step:(n + 1) * step] = part.astype(
                    jnp.bfloat16).reshape(2, cap, step)
            r_copy(k, half, g).start()

    def add(first, second):
        return (first.astype(jnp.float32) + second.astype(jnp.float32)).astype(jnp.bfloat16)

    def spread(k):
        for g in range(PIECES):
            z_land(k, g).wait_recv()
            x_copy(k, g).start()
            d_copy(k, g).start()

    def pass_on(k):
        for g in range(PIECES):
            x_land(k, g).wait_recv()
            e_copy(k, g).start()

    def far(k):
        for g in range(PIECES):
            e_land(k, g).wait_recv()
        compute(k, 1 - h)

    def near(k):
        for g in range(PIECES):
            d_land(k, g).wait_recv()
        compute(k, h)

    def join(k, half, g):
        cols = pl.ds(g * part_width, part_width)
        r_copy(k, half, g).wait_recv()
        cx[2 * k + half, :, cols] = add(po[4 * k + 2 * half + c, :, cols], rd[2 * k + half, :, cols])

    def give(k):
        for g in range(PIECES):
            join(k, 1 - h, g)
            v_copy(k, g).start()

    def finish(k):
        for g in range(PIECES):
            join(k, h, g)
            v_copy(k, g).wait_recv()
            cols = pl.ds(g * part_width, part_width)
            total = add(cx[2 * k + h, :, cols], rx[k, :, cols])

            @pl.when(k == 0)
            def _():
                ret[p, :, cols] = total

            @pl.when(k > 0)
            def _():
                fo[k, :, cols] = total
                w_copy(k, g).start()

    def stage(i, carry):
        for event, lag, first, last in PLAN:
            k = i - lag

            @pl.when((k >= first) & (k < experts + last))
            def _():
                event(k)

        return carry

    names_of = dict(spread=spread, pass_on=pass_on, far=far, near=near, give=give, finish=finish)
    PLAN = [(names_of[n], lag, first, last) for n, lag, first, last in SCHEDULE]

    for j in range(tiles):
        gate_copy(j).wait()
        up_copy(j).wait()
    down_copy.wait()
    lax.fori_loop(0, experts + STAGES, stage, 0)
    give(0)

    def settle(k, carry):
        for g in range(PIECES):
            x_copy(k, g).wait_send()
            d_copy(k, g).wait_send()
            e_copy(k, g).wait_send()
            r_copy(k, 0, g).wait_send()
            r_copy(k, 1, g).wait_send()
            v_copy(k, g).wait_send()

            @pl.when(k > 0)
            def _():
                z_copy(k, g).wait_send()
                w_copy(k, g).wait_send()

        return carry

    after = (col < row).astype(jnp.float32).astype(jnp.bfloat16)

    sides = jnp.concatenate(
        [ids_ref[...].astype(jnp.float32), weight_ref[...], jnp.zeros((LANE - 4, toks), jnp.float32)], axis=0).T

    def place_of(e, places):
        number = lax.convert_element_type(e, jnp.float32)
        hits = [(sides[:, n:n + 1] == number).astype(jnp.float32) for n in range(2)]
        rank = jnp.dot(
            after, jnp.broadcast_to(hits[0] + hits[1], (toks, LANE)).astype(jnp.bfloat16),
            preferred_element_type=jnp.float32)[:, 0:1]
        spot = rank + number * cap
        return tuple(old + hit * spot for old, hit in zip(places, hits))

    zero = jnp.zeros((toks, 1), jnp.float32)
    places = lax.fori_loop(0, experts, place_of, (zero, zero))
    lanes = lax.broadcasted_iota(jnp.int32, (toks, experts * cap), 1).astype(jnp.float32)
    picks = [(lanes == place).astype(jnp.float32).astype(jnp.bfloat16) for place in places]
    finish(experts - 1)
    finish(0)
    lax.fori_loop(0, experts, settle, 0)
    for g in range(PIECES):
        def landed(k, carry):
            w_land(k, g).wait_recv()
            return carry

        lax.fori_loop(1, experts, landed, 0)
        cols = pl.ds(g * part_width, part_width)
        rows = ret[:, :, cols].reshape(experts * cap, part_width)
        total = jnp.zeros((toks, part_width), jnp.float32)
        for m in range(2):
            total = total + sides[:, 2 + m:3 + m] * jnp.dot(
                picks[m], rows, preferred_element_type=jnp.float32)
        out_ref[:, cols] = total.astype(jnp.bfloat16)


def local(tokens, norm_gain, expert_ids, route_weights, w_gate, w_up, w_down):
    experts = lax.axis_size("ep") // 2
    toks, width = tokens.shape
    hidden = w_gate.shape[1]
    capacity = 2 * max(1, 5 * toks * expert_ids.shape[1] // (8 * experts))
    cap = -(-capacity // 16) * 16
    tiles = hidden // LANE
    kinds = -(-experts // 16) * 16
    any_space = pl.BlockSpec(memory_space=pl.ANY)
    dma = pltpu.SemaphoreType.DMA
    bf16 = jnp.bfloat16
    return pl.pallas_call(
        functools.partial(kernel, experts, cap),
        out_shape=pltpu.VMEM((toks, width), bf16),
        in_specs=[any_space] * 7,
        out_specs=pl.BlockSpec(memory_space=pltpu.VMEM),
        scratch_shapes=[
            pltpu.VMEM((toks, width), bf16),
            pltpu.VMEM((1, width), jnp.float32),
            pltpu.VMEM((2, toks), jnp.int32),
            pltpu.VMEM((2, toks), jnp.float32),
            pltpu.VMEM((toks, width), bf16),
            pltpu.VMEM((kinds, toks), jnp.float32),
            pltpu.VMEM((kinds, toks), jnp.float32),
            pltpu.VMEM((8, LANE), jnp.float32),
            pltpu.VMEM((experts, cap, width), bf16),
            pltpu.VMEM((experts * 4, cap, width), bf16),
            pltpu.VMEM((2 * cap, hidden), bf16),
            pltpu.VMEM((experts * 4, cap, width), bf16),
            pltpu.VMEM((experts * 2, cap, width), bf16),
            pltpu.VMEM((experts * 2, cap, width), bf16),
            pltpu.VMEM((experts, cap, width), bf16),
            pltpu.VMEM((experts, cap, width), bf16),
            pltpu.VMEM((experts, cap, width), bf16),
            pltpu.VMEM((tiles, width, 2 * LANE), bf16),
            pltpu.VMEM((hidden, width), bf16),
            dma((4,)), dma((tiles,)), dma((tiles,)), dma,
        ] + [dma((PIECES * experts,))] * 8 + [dma((2 * PIECES * experts,))] * 2 + [dma((PIECES * experts,))] * 4,
        compiler_params=pltpu.CompilerParams(
            collective_id=0, has_side_effects=True, vmem_limit_bytes=60 * 1024 * 1024),
    )(tokens, norm_gain.reshape(1, -1), expert_ids.T, route_weights.T, w_gate, w_up, w_down)


def solution(mesh):
    placed = (
        P(("grp", "ep", "tp"), None),
        P(),
        P(("grp", "ep", "tp"), None),
        P(("grp", "ep", "tp"), None),
        P(None, ("ep", "tp")),
        P(None, ("ep", "tp")),
        P(("ep", "tp"), None),
    )
    return jax.shard_map(
        local, mesh=mesh, in_specs=placed, out_specs=P(("grp", "ep", "tp"), None), check_vma=False
    )
```

```python
import functools

import jax
import jax.numpy as jnp
from jax import lax
from jax.experimental import pallas as pl
from jax.experimental.pallas import tpu as pltpu
from jax.sharding import PartitionSpec as P

MESH = pl.DeviceIdType.MESH
LANE = 128
PIECES = 2
TURNS = ((0, 2, 3, 1), (0, 3, 2, 1))
SENDS = (
    ((2, 1), (2, 0), (1, 1), (1, 0), (3, 1), (3, 0)),
    ((3, 1), (2, 0), (2, 1), (3, 0), (1, 0), (1, 1)),
)
ORDER = (
    ("spread", 2, 1),
    ("spread", 2, 0),
    ("spread", 3, 1),
    ("near", 2),
    ("spread", 3, 0),
    ("pass_on", 2, 0),
    ("pass_on", 2, 1),
    ("spread", 1, 0),
    ("far", 2),
    ("spread", 1, 1),
    ("give", 2, 0),
    ("pass_on", 3, 1),
    ("pass_on", 3, 0),
    ("near", 3),
    ("pass_on", 0, 1),
    ("far", 3),
    ("give", 2, 1),
    ("pass_on", 1, 1),
    ("give", 3, 1),
    ("pass_on", 1, 0),
    ("finish", 2, 0),
    ("pass_on", 0, 0),
    ("far", 1),
    ("finish", 2, 1),
    ("give", 3, 0),
    ("far", 0),
    ("finish", 3, 1),
    ("give", 1, 1),
    ("give", 1, 0),
    ("near", 1),
    ("give", 0, 1),
    ("finish", 3, 0),
    ("finish", 1, 1),
    ("give", 0, 0),
    ("near", 0),
    ("finish", 1, 0),
    ("finish", 0, 1),
    ("finish", 0, 0),
)


def mix_index(first, second, count):
    total = first * 0
    bit = 1
    while bit < count:
        one, two = (first // bit) % 2, (second // bit) % 2
        total = total + bit * (one + two - 2 * one * two)
        bit *= 2
    return total


def kernel(
    experts, cap,
    tok_hbm, gain_hbm, ids_hbm, weight_hbm, gate_ref, up_ref, down_ref,
    out_ref,
    tok_ref, gain_ref, ids_ref, weight_ref, norm, names, ranks, sides, picks, xs, xa, hid, po, rd, cx, rx, fo, ret, wgu, wd,
    in_sem, gate_sem, up_sem, down_sem,
    z_send, z_recv, x_send, x_recv, d_send, d_recv, e_send, e_recv,
    r_send, r_recv, v_send, v_recv, w_send, w_recv,
):
    ep, c = lax.axis_index("ep"), lax.axis_index("tp")
    p, h = ep // 2, ep % 2
    toks, width = tok_ref.shape
    tiles = wgu.shape[0]
    part_width = width // PIECES
    across = {"ep": 2 * p + 1 - h, "tp": c}
    beside = {"ep": ep, "tp": 1 - c}

    def plane(q):
        return {"ep": 2 * q + h, "tp": c}

    loads = [
        pltpu.make_async_copy(src, dst, in_sem.at[n]) for n, (src, dst) in enumerate((
            (tok_hbm, tok_ref), (gain_hbm, gain_ref), (ids_hbm, ids_ref), (weight_hbm, weight_ref)))]
    for load in loads:
        load.start()

    barrier = pltpu.get_barrier_semaphore()

    def greet(k, carry):
        pl.semaphore_signal(barrier, inc=1, device_id=plane(mix_index(p, k, experts)), device_id_type=MESH)
        return carry

    lax.fori_loop(1, experts, greet, 0)
    pl.semaphore_signal(barrier, inc=1, device_id=across, device_id_type=MESH)
    pl.semaphore_signal(barrier, inc=1, device_id=beside, device_id_type=MESH)

    def gate_copy(j):
        return pltpu.make_async_copy(
            gate_ref.at[:, pl.ds(j * LANE, LANE)], wgu.at[j, :, pl.ds(0, LANE)], gate_sem.at[j])

    def up_copy(j):
        return pltpu.make_async_copy(
            up_ref.at[:, pl.ds(j * LANE, LANE)], wgu.at[j, :, pl.ds(LANE, LANE)], up_sem.at[j])

    down_copy = pltpu.make_async_copy(down_ref, wd, down_sem)
    for j in range(tiles):
        gate_copy(j).start()
        up_copy(j).start()
    down_copy.start()

    row = lax.broadcasted_iota(jnp.int32, (toks, toks), 0)
    col = lax.broadcasted_iota(jnp.int32, (toks, toks), 1)
    before = (row < col).astype(jnp.float32).astype(jnp.bfloat16)
    slots = lax.broadcasted_iota(jnp.int32, (cap, toks), 0).astype(jnp.float32)
    for load in loads[1:]:
        load.wait()
    kinds = lax.broadcasted_iota(jnp.int32, names.shape, 0)
    names[...] = ((ids_ref[0:1, :] == kinds) | (ids_ref[1:2, :] == kinds)).astype(jnp.float32)
    ranks[...] = jnp.dot(names[...].astype(jnp.bfloat16), before, preferred_element_type=jnp.float32)

    loads[0].wait()
    values = tok_ref[...].astype(jnp.float32)
    scale_rows = lax.rsqrt(jnp.mean(values * values, axis=1, keepdims=True) + 1e-06)
    norm[...] = (values * scale_rows * gain_ref[...]).astype(jnp.bfloat16)

    def remote(src, dst, send, recv, target):
        return pltpu.make_async_remote_copy(
            src_ref=src, dst_ref=dst, send_sem=send, recv_sem=recv, device_id=target, device_id_type=MESH)

    def cut(ref, index, g):
        return ref.at[index, :, pl.ds(g * part_width, part_width)]

    def z_pair(k, g, origin):
        q = mix_index(p, k, experts)
        n = PIECES * k + g
        return remote(
            cut(xs, q, g), cut(xa, 4 * origin(q) + 2 * h + c, g), z_send.at[n], z_recv.at[n], plane(q))

    def z_copy(k, g):
        return z_pair(k, g, lambda q: p)

    def z_land(k, g):
        return z_pair(k, g, lambda q: q)

    def mine(k, half, core, g):
        return cut(xa, 4 * mix_index(p, k, experts) + 2 * half + core, g)

    def shift(k, g, there, here, send, recv, target):
        n = PIECES * k + g
        return remote(mine(k, *there, g), mine(k, *here, g), send.at[n], recv.at[n], target)

    def x_copy(k, g):
        return shift(k, g, (h, c), (h, c), x_send, x_recv, across)

    def x_land(k, g):
        return shift(k, g, (h, c), (1 - h, c), x_send, x_recv, across)

    def d_copy(k, g):
        return shift(k, g, (h, c), (h, c), d_send, d_recv, beside)

    def d_land(k, g):
        return shift(k, g, (h, c), (h, 1 - c), d_send, d_recv, beside)

    def e_copy(k, g):
        return shift(k, g, (1 - h, c), (1 - h, c), e_send, e_recv, beside)

    def e_land(k, g):
        return shift(k, g, (1 - h, c), (1 - h, 1 - c), e_send, e_recv, beside)

    def r_copy(k, half, g):
        n = 2 * (PIECES * k + g) + half
        return remote(
            cut(po, 4 * k + 2 * half + 1 - c, g), cut(rd, 2 * k + half, g),
            r_send.at[n], r_recv.at[n], beside)

    def v_copy(k, g):
        n = PIECES * k + g
        return remote(cut(cx, k, g), cut(rx, k, g), v_send.at[n], v_recv.at[n], across)

    def w_pair(k, g, origin):
        q = mix_index(p, k, experts)
        n = PIECES * k + g
        return remote(cut(fo, k, g), cut(ret, origin(q), g), w_send.at[n], w_recv.at[n], plane(q))

    def w_copy(k, g):
        return w_pair(k, g, lambda q: p)

    def w_land(k, g):
        return w_pair(k, g, lambda q: q)

    def picked(e):
        spot = pl.ds(e, 1)
        pick = jnp.where(slots == ranks[spot, :], names[spot, :], 0.0).astype(jnp.bfloat16)
        return jnp.dot(pick, norm[...], preferred_element_type=jnp.float32).astype(jnp.bfloat16)

    inner = (p + 1) // 2 % 2

    def turn(s):
        outside, inside = TURNS[0][s], TURNS[1][s]
        return outside if outside == inside else outside + inner * (inside - outside)

    pl.semaphore_wait(barrier, experts + 1)

    xa[4 * p + 2 * h + c] = picked(p)
    for g in range(PIECES):
        x_copy(0, g).start()
        d_copy(0, g).start()

    if experts == len(TURNS[0]):
        for k in range(1, experts):
            xs[mix_index(p, k, experts)] = picked(mix_index(p, k, experts))
        for side, sends in enumerate(SENDS):
            @pl.when(inner == side)
            def _():
                for s, g in sends:
                    z_copy(TURNS[side][s], g).start()
    else:
        def fill(k, carry):
            e = mix_index(p, k, experts)
            xs[e] = picked(e)
            for g in range(PIECES):
                z_copy(k, g).start()
            return carry

        lax.fori_loop(1, experts, fill, 0)

    step = 2 * LANE

    def compute(k, half):
        rows = xa[pl.ds(4 * mix_index(p, k, experts) + 2 * half, 2)].reshape(2 * cap, width)
        for j in range(tiles):
            both = jnp.dot(rows, wgu[j], preferred_element_type=jnp.float32)
            gate, up = both[:, :LANE], both[:, LANE:]
            hid[:, j * LANE:(j + 1) * LANE] = (gate / (1.0 + jnp.exp(-gate)) * up).astype(jnp.bfloat16)
        many = part_width // step
        for g in range(PIECES):
            for n in range(g * many, (g + 1) * many):
                part = jnp.dot(hid[...], wd[:, n * step:(n + 1) * step], preferred_element_type=jnp.float32)
                po[pl.ds(4 * k + 2 * half, 2), :, n * step:(n + 1) * step] = part.astype(
                    jnp.bfloat16).reshape(2, cap, step)
            r_copy(k, half, g).start()

    def add(first, second):
        return (first.astype(jnp.float32) + second.astype(jnp.float32)).astype(jnp.bfloat16)

    def spread(k, g):
        z_land(k, g).wait_recv()
        x_copy(k, g).start()
        d_copy(k, g).start()

    def pass_on(k, g):
        x_land(k, g).wait_recv()
        e_copy(k, g).start()

    def far(k):
        for g in range(PIECES):
            e_land(k, g).wait_recv()
        compute(k, 1 - h)

    def near(k):
        for g in range(PIECES):
            d_land(k, g).wait_recv()
        compute(k, h)

    def joined(k, half, g):
        cols = pl.ds(g * part_width, part_width)
        r_copy(k, half, g).wait_recv()
        return add(po[4 * k + 2 * half + c, :, cols], rd[2 * k + half, :, cols])

    def give(k, g):
        cx[k, :, g * part_width:(g + 1) * part_width] = joined(k, 1 - h, g)
        v_copy(k, g).start()

    def finish(k, g):
        cols = pl.ds(g * part_width, part_width)
        here = joined(k, h, g)
        v_copy(k, g).wait_recv()
        total = add(here, rx[k, :, cols])
        if isinstance(k, int) and k == 0:
            ret[p, :, cols] = total
        else:
            fo[k, :, cols] = total
            w_copy(k, g).start()

    after = (col < row).astype(jnp.float32).astype(jnp.bfloat16)

    sides[...] = jnp.concatenate(
        [ids_ref[...].astype(jnp.float32), weight_ref[...], jnp.zeros((LANE - 4, toks), jnp.float32)], axis=0).T

    def place_of(e, places):
        number = lax.convert_element_type(e, jnp.float32)
        hits = [(sides[:, n:n + 1] == number).astype(jnp.float32) for n in range(2)]
        rank = jnp.dot(
            after, jnp.broadcast_to(hits[0] + hits[1], (toks, LANE)).astype(jnp.bfloat16),
            preferred_element_type=jnp.float32)[:, 0:1]
        spot = rank + number * cap
        return tuple(old + hit * spot for old, hit in zip(places, hits))

    zero = jnp.zeros((toks, 1), jnp.float32)
    places = lax.fori_loop(0, experts, place_of, (zero, zero))
    lanes = lax.broadcasted_iota(jnp.int32, (toks, experts * cap), 1).astype(jnp.float32)
    for m in range(2):
        picks[m] = (lanes == places[m]).astype(jnp.float32).astype(jnp.bfloat16)

    for j in range(tiles):
        gate_copy(j).wait()
        up_copy(j).wait()
    down_copy.wait()

    events = dict(spread=spread, pass_on=pass_on, far=far, near=near, give=give, finish=finish)
    if experts == len(TURNS[0]):
        for name, s, *g in ORDER:
            events[name](turn(s), *g)
    else:
        def each(event, k):
            for g in range(PIECES):
                event(k, g)

        def stage(k, carry):
            near(k)

            @pl.when(k + 1 < experts)
            def _():
                each(spread, k + 1)

            each(pass_on, k)
            far(k)

            @pl.when(k > 1)
            def _():
                each(finish, k - 1)

            @pl.when(k > 0)
            def _():
                each(give, k)

            return carry

        lax.fori_loop(0, experts, stage, 0)
        each(give, 0)
        each(finish, experts - 1)
        each(finish, 0)

    def settle(k, carry):
        for g in range(PIECES):
            x_copy(k, g).wait_send()
            d_copy(k, g).wait_send()
            e_copy(k, g).wait_send()
            r_copy(k, 0, g).wait_send()
            r_copy(k, 1, g).wait_send()
            v_copy(k, g).wait_send()

            @pl.when(k > 0)
            def _():
                z_copy(k, g).wait_send()
                w_copy(k, g).wait_send()

        return carry

    for g in range(PIECES):
        def landed(k, carry):
            w_land(k, g).wait_recv()
            return carry

        lax.fori_loop(1, experts, landed, 0)
        cols = pl.ds(g * part_width, part_width)
        rows = ret[:, :, cols].reshape(experts * cap, part_width)
        total = jnp.zeros((toks, part_width), jnp.float32)
        for m in range(2):
            total = total + sides[:, 2 + m:3 + m] * jnp.dot(
                picks[m], rows, preferred_element_type=jnp.float32)
        out_ref[:, cols] = total.astype(jnp.bfloat16)
    lax.fori_loop(0, experts, settle, 0)


def local(tokens, norm_gain, expert_ids, route_weights, w_gate, w_up, w_down):
    experts = lax.axis_size("ep") // 2
    toks, width = tokens.shape
    hidden = w_gate.shape[1]
    capacity = 2 * max(1, 5 * toks * expert_ids.shape[1] // (8 * experts))
    cap = -(-capacity // 16) * 16
    tiles = hidden // LANE
    kinds = -(-experts // 16) * 16
    any_space = pl.BlockSpec(memory_space=pl.ANY)
    dma = pltpu.SemaphoreType.DMA
    bf16 = jnp.bfloat16
    return pl.pallas_call(
        functools.partial(kernel, experts, cap),
        out_shape=pltpu.VMEM((toks, width), bf16),
        in_specs=[any_space] * 7,
        out_specs=pl.BlockSpec(memory_space=pltpu.VMEM),
        scratch_shapes=[
            pltpu.VMEM((toks, width), bf16),
            pltpu.VMEM((1, width), jnp.float32),
            pltpu.VMEM((2, toks), jnp.int32),
            pltpu.VMEM((2, toks), jnp.float32),
            pltpu.VMEM((toks, width), bf16),
            pltpu.VMEM((kinds, toks), jnp.float32),
            pltpu.VMEM((kinds, toks), jnp.float32),
            pltpu.VMEM((toks, LANE), jnp.float32),
            pltpu.VMEM((2, toks, experts * cap), bf16),
            pltpu.VMEM((experts, cap, width), bf16),
            pltpu.VMEM((experts * 4, cap, width), bf16),
            pltpu.VMEM((2 * cap, hidden), bf16),
            pltpu.VMEM((experts * 4, cap, width), bf16),
            pltpu.VMEM((experts * 2, cap, width), bf16),
            pltpu.VMEM((experts, cap, width), bf16),
            pltpu.VMEM((experts, cap, width), bf16),
            pltpu.VMEM((experts, cap, width), bf16),
            pltpu.VMEM((experts, cap, width), bf16),
            pltpu.VMEM((tiles, width, 2 * LANE), bf16),
            pltpu.VMEM((hidden, width), bf16),
            dma((4,)), dma((tiles,)), dma((tiles,)), dma,
        ] + [dma((PIECES * experts,))] * 8 + [dma((2 * PIECES * experts,))] * 2 + [dma((PIECES * experts,))] * 4,
        compiler_params=pltpu.CompilerParams(
            collective_id=0, has_side_effects=True, vmem_limit_bytes=60 * 1024 * 1024),
    )(tokens, norm_gain.reshape(1, -1), expert_ids.T, route_weights.T, w_gate, w_up, w_down)


def solution(mesh):
    placed = (
        P(("grp", "ep", "tp"), None),
        P(),
        P(("grp", "ep", "tp"), None),
        P(("grp", "ep", "tp"), None),
        P(None, ("ep", "tp")),
        P(None, ("ep", "tp")),
        P(("ep", "tp"), None),
    )
    return jax.shard_map(
        local, mesh=mesh, in_specs=placed, out_specs=P(("grp", "ep", "tp"), None), check_vma=False
    )
```

```python
import functools

import jax
import jax.numpy as jnp
from jax import lax
from jax.experimental import pallas as pl
from jax.experimental.pallas import tpu as pltpu
from jax.sharding import PartitionSpec as P

MESH = pl.DeviceIdType.MESH
LANE = 128
PIECES = 2
TURNS = ((0, 2, 1, 3), (0, 3, 1, 2))
SENDS = (
    ((3, 0), (3, 1), (1, 0), (1, 1), (2, 1), (2, 0)),
    ((3, 1), (2, 1), (1, 1), (2, 0), (3, 0), (1, 0)),
)
ORDER = (
    ("spread", 3, 0),
    ("spread", 3, 1),
    ("spread", 2, 1),
    ("pass_on", 0, 0),
    ("pass_on", 3, 0),
    ("pass_on", 0, 1),
    ("pass_on", 3, 1),
    ("spread", 2, 0),
    ("far", 3),
    ("pass_on", 2, 1),
    ("spread", 1, 1),
    ("near", 2),
    ("give", 3, 1),
    ("pass_on", 2, 0),
    ("near", 3),
    ("spread", 1, 0),
    ("give", 3, 0),
    ("pass_on", 1, 1),
    ("far", 2),
    ("near", 1),
    ("finish", 3, 1),
    ("give", 2, 0),
    ("pass_on", 1, 0),
    ("far", 0),
    ("finish", 3, 0),
    ("give", 2, 1),
    ("far", 1),
    ("finish", 2, 0),
    ("give", 1, 0),
    ("give", 1, 1),
    ("near", 0),
    ("finish", 2, 1),
    ("finish", 1, 0),
    ("give", 0, 0),
    ("give", 0, 1),
    ("finish", 1, 1),
    ("finish", 0, 0),
    ("finish", 0, 1),
)


def mix_index(first, second, count):
    total = first * 0
    bit = 1
    while bit < count:
        one, two = (first // bit) % 2, (second // bit) % 2
        total = total + bit * (one + two - 2 * one * two)
        bit *= 2
    return total


def kernel(
    experts, cap,
    tok_hbm, gain_hbm, ids_hbm, weight_hbm, gate_ref, up_ref, down_ref,
    out_ref,
    tok_ref, gain_ref, ids_ref, weight_ref, norm, names, ranks, sides, picks, xs, xa, hid, po, rd, cx, rx, fo, ret, wgu, wd,
    in_sem, wgu_sem, wd_sem,
    z_send, z_recv, x_send, x_recv, d_send, d_recv, e_send, e_recv,
    r_send, r_recv, v_send, v_recv, w_send, w_recv,
):
    ep, c = lax.axis_index("ep"), lax.axis_index("tp")
    p, h = ep // 2, ep % 2
    toks, width = tok_ref.shape
    tiles = wgu.shape[0]
    part_width = width // PIECES
    across = {"ep": 2 * p + 1 - h, "tp": c}
    beside = {"ep": ep, "tp": 1 - c}

    def plane(q):
        return {"ep": 2 * q + h, "tp": c}

    loads = [
        pltpu.make_async_copy(src, dst, in_sem.at[n]) for n, (src, dst) in enumerate((
            (tok_hbm, tok_ref), (gain_hbm, gain_ref), (ids_hbm, ids_ref), (weight_hbm, weight_ref)))]
    for load in loads:
        load.start()

    barrier = pltpu.get_barrier_semaphore()

    def greet(k, carry):
        pl.semaphore_signal(barrier, inc=1, device_id=plane(mix_index(p, k, experts)), device_id_type=MESH)
        return carry

    lax.fori_loop(1, experts, greet, 0)
    pl.semaphore_signal(barrier, inc=1, device_id=across, device_id_type=MESH)
    pl.semaphore_signal(barrier, inc=1, device_id=beside, device_id_type=MESH)

    def gate_copy(j):
        return pltpu.make_async_copy(
            gate_ref.at[:, pl.ds(j * LANE, LANE)], wgu.at[j, :, pl.ds(0, LANE)], wgu_sem)

    def up_copy(j):
        return pltpu.make_async_copy(
            up_ref.at[:, pl.ds(j * LANE, LANE)], wgu.at[j, :, pl.ds(LANE, LANE)], wgu_sem)

    down_copy = pltpu.make_async_copy(down_ref, wd, wd_sem)
    for j in range(tiles):
        gate_copy(j).start()
        up_copy(j).start()
    down_copy.start()

    row = lax.broadcasted_iota(jnp.int32, (toks, toks), 0)
    col = lax.broadcasted_iota(jnp.int32, (toks, toks), 1)
    before = (row < col).astype(jnp.float32).astype(jnp.bfloat16)
    slots = lax.broadcasted_iota(jnp.int32, (cap, toks), 0).astype(jnp.float32)
    for load in loads[1:]:
        load.wait()
    kinds = lax.broadcasted_iota(jnp.int32, names.shape, 0)
    names[...] = ((ids_ref[0:1, :] == kinds) | (ids_ref[1:2, :] == kinds)).astype(jnp.float32)
    ranks[...] = jnp.dot(names[...].astype(jnp.bfloat16), before, preferred_element_type=jnp.float32)

    loads[0].wait()
    values = tok_ref[...].astype(jnp.float32)
    scale_rows = lax.rsqrt(jnp.mean(values * values, axis=1, keepdims=True) + 1e-06)
    norm[...] = (values * scale_rows * gain_ref[...]).astype(jnp.bfloat16)

    def remote(src, dst, send, recv, target):
        return pltpu.make_async_remote_copy(
            src_ref=src, dst_ref=dst, send_sem=send, recv_sem=recv, device_id=target, device_id_type=MESH)

    def cut(ref, index, g):
        return ref.at[index, :, pl.ds(g * part_width, part_width)]

    def z_pair(k, g, origin):
        q = mix_index(p, k, experts)
        n = PIECES * (k - 1) + g
        return remote(
            cut(xs, q, g), cut(xa, 4 * origin(q) + 2 * h + c, g), z_send, z_recv.at[n], plane(q))

    def z_copy(k, g):
        return z_pair(k, g, lambda q: p)

    def z_land(k, g):
        return z_pair(k, g, lambda q: q)

    def mine(k, half, core, g):
        return cut(xa, 4 * mix_index(p, k, experts) + 2 * half + core, g)

    def x_copy(k, g):
        return remote(mine(k, h, c, g), mine(k, h, c, g), x_send, x_recv.at[PIECES * k + g], across)

    def x_land(k, g):
        return remote(mine(k, h, c, g), mine(k, 1 - h, c, g), x_send, x_recv.at[PIECES * k + g], across)

    def d_copy(k, g):
        return remote(mine(k, h, c, g), mine(k, h, c, g), d_send, d_recv.at[k], beside)

    def e_copy(k, g):
        return remote(mine(k, 1 - h, c, g), mine(k, 1 - h, c, g), e_send, e_recv.at[k], beside)

    def landing(k, half, send, recv):
        first = 4 * mix_index(p, k, experts) + 2 * half
        return remote(xa.at[first + c], xa.at[first + 1 - c], send, recv.at[k], beside)

    def r_copy(k, half, g):
        n = 2 * (PIECES * k + g) + half
        return remote(
            cut(po, 4 * k + 2 * half + 1 - c, g), cut(rd, 2 * k + half, g),
            r_send, r_recv.at[n], beside)

    def v_copy(k, g):
        n = PIECES * k + g
        return remote(cut(cx, k, g), cut(rx, k, g), v_send, v_recv.at[n], across)

    def w_copy(k, g):
        q = mix_index(p, k, experts)
        return remote(cut(fo, k, g), cut(ret, p, g), w_send, w_recv.at[g], plane(q))

    def w_land(g):
        cols = pl.ds(g * part_width, part_width)
        return remote(
            fo.at[pl.ds(0, experts - 1), :, cols], ret.at[pl.ds(0, experts - 1), :, cols],
            w_send, w_recv.at[g], beside)

    def picked(e):
        spot = pl.ds(e, 1)
        pick = jnp.where(slots == ranks[spot, :], names[spot, :], 0.0).astype(jnp.bfloat16)
        return jnp.dot(pick, norm[...], preferred_element_type=jnp.float32).astype(jnp.bfloat16)

    inner = (p + 1) // 2 % 2

    def turn(s):
        outside, inside = TURNS[0][s], TURNS[1][s]
        return outside if outside == inside else outside + inner * (inside - outside)

    pl.semaphore_wait(barrier, experts + 1)

    xa[4 * p + 2 * h + c] = picked(p)
    for g in range(PIECES):
        x_copy(0, g).start()
        d_copy(0, g).start()

    if experts == len(TURNS[0]):
        for k in range(1, experts):
            xs[mix_index(p, k, experts)] = picked(mix_index(p, k, experts))
        for side, sends in enumerate(SENDS):
            @pl.when(inner == side)
            def _():
                for s, g in sends:
                    z_copy(TURNS[side][s], g).start()
    else:
        def fill(k, carry):
            e = mix_index(p, k, experts)
            xs[e] = picked(e)
            for g in range(PIECES):
                z_copy(k, g).start()
            return carry

        lax.fori_loop(1, experts, fill, 0)

    step = 2 * LANE

    def compute(k, half):
        rows = xa[pl.ds(4 * mix_index(p, k, experts) + 2 * half, 2)].reshape(2 * cap, width)
        for j in range(tiles):
            both = jnp.dot(rows, wgu[j], preferred_element_type=jnp.float32)
            gate, up = both[:, :LANE], both[:, LANE:]
            hid[:, j * LANE:(j + 1) * LANE] = (gate / (1.0 + jnp.exp(-gate)) * up).astype(jnp.bfloat16)
        many = part_width // step
        for g in range(PIECES):
            for n in range(g * many, (g + 1) * many):
                part = jnp.dot(hid[...], wd[:, n * step:(n + 1) * step], preferred_element_type=jnp.float32)
                po[pl.ds(4 * k + 2 * half, 2), :, n * step:(n + 1) * step] = part.astype(
                    jnp.bfloat16).reshape(2, cap, step)
            r_copy(k, half, g).start()

    def add(first, second):
        return (first.astype(jnp.float32) + second.astype(jnp.float32)).astype(jnp.bfloat16)

    def spread(k, g):
        z_land(k, g).wait_recv()
        x_copy(k, g).start()
        d_copy(k, g).start()

    def pass_on(k, g):
        x_land(k, g).wait_recv()
        e_copy(k, g).start()

    def far(k):
        landing(k, 1 - h, e_send, e_recv).wait_recv()
        compute(k, 1 - h)

    def near(k):
        landing(k, h, d_send, d_recv).wait_recv()
        compute(k, h)

    def joined(k, half, g):
        cols = pl.ds(g * part_width, part_width)
        r_copy(k, half, g).wait_recv()
        return add(po[4 * k + 2 * half + c, :, cols], rd[2 * k + half, :, cols])

    def give(k, g):
        cx[k, :, g * part_width:(g + 1) * part_width] = joined(k, 1 - h, g)
        v_copy(k, g).start()

    def finish(k, g):
        cols = pl.ds(g * part_width, part_width)
        here = joined(k, h, g)
        v_copy(k, g).wait_recv()
        total = add(here, rx[k, :, cols])
        if isinstance(k, int) and k == 0:
            ret[p, :, cols] = total
        else:
            fo[k, :, cols] = total
            w_copy(k, g).start()

    after = (col < row).astype(jnp.float32).astype(jnp.bfloat16)

    sides[...] = jnp.concatenate(
        [ids_ref[...].astype(jnp.float32), weight_ref[...], jnp.zeros((LANE - 4, toks), jnp.float32)], axis=0).T

    def place_of(e, places):
        number = lax.convert_element_type(e, jnp.float32)
        hits = [(sides[:, n:n + 1] == number).astype(jnp.float32) for n in range(2)]
        rank = jnp.dot(
            after, jnp.broadcast_to(hits[0] + hits[1], (toks, LANE)).astype(jnp.bfloat16),
            preferred_element_type=jnp.float32)[:, 0:1]
        spot = rank + number * cap
        return tuple(old + hit * spot for old, hit in zip(places, hits))

    zero = jnp.zeros((toks, 1), jnp.float32)
    places = lax.fori_loop(0, experts, place_of, (zero, zero))
    lanes = lax.broadcasted_iota(jnp.int32, (toks, experts * cap), 1).astype(jnp.float32)
    for m in range(2):
        picks[m] = (lanes == places[m]).astype(jnp.float32).astype(jnp.bfloat16)

    pltpu.make_async_copy(wgu, wgu, wgu_sem).wait()
    down_copy.wait()

    def sent(ref, count, send, recv):
        part = ref.at[pl.ds(0, count)]
        remote(part, part, send, recv.at[0], beside).wait_send()

    def settle():
        sent(xs, experts - 1, z_send, z_recv)
        sent(xa, experts, x_send, x_recv)
        sent(xa, experts, d_send, d_recv)
        sent(xa, experts, e_send, e_recv)
        sent(po, 2 * experts, r_send, r_recv)

    events = dict(spread=spread, pass_on=pass_on, far=far, near=near, give=give, finish=finish)
    if experts == len(TURNS[0]):
        for name, s, *g in ORDER[:-1]:
            events[name](turn(s), *g)
        settle()
        for name, s, *g in ORDER[-1:]:
            events[name](turn(s), *g)
    else:
        def each(event, k):
            for g in range(PIECES):
                event(k, g)

        def stage(k, carry):
            near(k)

            @pl.when(k + 1 < experts)
            def _():
                each(spread, k + 1)

            each(pass_on, k)
            far(k)

            @pl.when(k > 1)
            def _():
                each(finish, k - 1)

            @pl.when(k > 0)
            def _():
                each(give, k)

            return carry

        lax.fori_loop(0, experts, stage, 0)
        each(give, 0)
        each(finish, experts - 1)
        settle()
        each(finish, 0)

    for g in range(PIECES):
        w_land(g).wait_recv()
        cols = pl.ds(g * part_width, part_width)
        rows = ret[:, :, cols].reshape(experts * cap, part_width)
        total = jnp.zeros((toks, part_width), jnp.float32)
        for m in range(2):
            total = total + sides[:, 2 + m:3 + m] * jnp.dot(
                picks[m], rows, preferred_element_type=jnp.float32)
        out_ref[:, cols] = total.astype(jnp.bfloat16)
    sent(cx, experts, v_send, v_recv)
    sent(fo, experts - 1, w_send, w_recv)


def local(tokens, norm_gain, expert_ids, route_weights, w_gate, w_up, w_down):
    experts = lax.axis_size("ep") // 2
    toks, width = tokens.shape
    hidden = w_gate.shape[1]
    capacity = 2 * max(1, 5 * toks * expert_ids.shape[1] // (8 * experts))
    cap = -(-capacity // 16) * 16
    tiles = hidden // LANE
    kinds = -(-experts // 16) * 16
    any_space = pl.BlockSpec(memory_space=pl.ANY)
    dma = pltpu.SemaphoreType.DMA
    bf16 = jnp.bfloat16
    return pl.pallas_call(
        functools.partial(kernel, experts, cap),
        out_shape=pltpu.VMEM((toks, width), bf16),
        in_specs=[any_space] * 7,
        out_specs=pl.BlockSpec(memory_space=pltpu.VMEM),
        scratch_shapes=[
            pltpu.VMEM((toks, width), bf16),
            pltpu.VMEM((1, width), jnp.float32),
            pltpu.VMEM((2, toks), jnp.int32),
            pltpu.VMEM((2, toks), jnp.float32),
            pltpu.VMEM((toks, width), bf16),
            pltpu.VMEM((kinds, toks), jnp.float32),
            pltpu.VMEM((kinds, toks), jnp.float32),
            pltpu.VMEM((toks, LANE), jnp.float32),
            pltpu.VMEM((2, toks, experts * cap), bf16),
            pltpu.VMEM((experts, cap, width), bf16),
            pltpu.VMEM((experts * 4, cap, width), bf16),
            pltpu.VMEM((2 * cap, hidden), bf16),
            pltpu.VMEM((experts * 4, cap, width), bf16),
            pltpu.VMEM((experts * 2, cap, width), bf16),
            pltpu.VMEM((experts, cap, width), bf16),
            pltpu.VMEM((experts, cap, width), bf16),
            pltpu.VMEM((experts, cap, width), bf16),
            pltpu.VMEM((experts, cap, width), bf16),
            pltpu.VMEM((tiles, width, 2 * LANE), bf16),
            pltpu.VMEM((hidden, width), bf16),
            dma((4,)), dma, dma,
            dma, dma((PIECES * (experts - 1),)), dma, dma((PIECES * experts,)),
            dma, dma((experts,)), dma, dma((experts,)),
            dma, dma((2 * PIECES * experts,)), dma, dma((PIECES * experts,)), dma, dma((PIECES,)),
        ],
        compiler_params=pltpu.CompilerParams(
            collective_id=0, has_side_effects=True, vmem_limit_bytes=60 * 1024 * 1024),
    )(tokens, norm_gain.reshape(1, -1), expert_ids.T, route_weights.T, w_gate, w_up, w_down)


def solution(mesh):
    placed = (
        P(("grp", "ep", "tp"), None),
        P(),
        P(("grp", "ep", "tp"), None),
        P(("grp", "ep", "tp"), None),
        P(None, ("ep", "tp")),
        P(None, ("ep", "tp")),
        P(("ep", "tp"), None),
    )
    return jax.shard_map(
        local, mesh=mesh, in_specs=placed, out_specs=P(("grp", "ep", "tp"), None), check_vma=False
    )
```

```python
import functools

import jax
import jax.numpy as jnp
from jax import lax
from jax.experimental import pallas as pl
from jax.experimental.pallas import tpu as pltpu
from jax.sharding import PartitionSpec as P

MESH = pl.DeviceIdType.MESH
LANE = 128
PIECES = 4
TURNS = ((0, 1, 3, 2), (0, 3, 2, 1))
SENDS = (
    (
        (2, 3),
        (1, 1),
        (3, 1),
        (1, 0),
        (3, 2),
        (3, 3),
        (3, 0),
        (2, 2),
        (2, 0),
        (2, 1),
        (1, 3),
        (1, 2),
    ),
    (
        (2, 2),
        (3, 1),
        (1, 1),
        (3, 3),
        (1, 3),
        (2, 0),
        (3, 2),
        (2, 1),
        (2, 3),
        (3, 0),
        (1, 0),
        (1, 2),
    ),
)
ORDERS = (
    (
        ("near", 0),
        ("pass_on", 0, 0),
        ("spread", 1, 1),
        ("spread", 2, 3),
        ("pass_on", 0, 3),
        ("spread", 3, 2),
        ("pass_on", 0, 1),
        ("pass_on", 0, 2),
        ("spread", 1, 0),
        ("spread", 1, 2),
        ("spread", 1, 3),
        ("far", 0),
        ("spread", 2, 2),
        ("spread", 2, 0),
        ("spread", 2, 1),
        ("pass_on", 2, 2),
        ("give", 0, 1),
        ("spread", 3, 0),
        ("pass_on", 1, 1),
        ("pass_on", 2, 3),
        ("pass_on", 2, 1),
        ("pass_on", 2, 0),
        ("spread", 3, 1),
        ("spread", 3, 3),
        ("far", 2),
        ("give", 2, 0),
        ("pass_on", 1, 0),
        ("give", 0, 0),
        ("pass_on", 3, 0),
        ("pass_on", 1, 2),
        ("pass_on", 3, 1),
        ("pass_on", 3, 2),
        ("pass_on", 1, 3),
        ("give", 2, 1),
        ("near", 2),
        ("pass_on", 3, 3),
        ("give", 2, 2),
        ("give", 2, 3),
        ("finish", 2, 0),
        ("far", 3),
        ("finish", 2, 1),
        ("give", 3, 0),
        ("near", 3),
        ("finish", 2, 2),
        ("give", 3, 2),
        ("give", 3, 3),
        ("finish", 0, 1),
        ("finish", 2, 3),
        ("far", 1),
        ("finish", 3, 0),
        ("give", 3, 1),
        ("give", 1, 0),
        ("give", 1, 2),
        ("give", 1, 3),
        ("finish", 3, 2),
        ("give", 1, 1),
        ("give", 0, 3),
        ("finish", 0, 0),
        ("finish", 3, 3),
        ("near", 1),
        ("give", 0, 2),
        ("finish", 3, 1),
        ("finish", 1, 0),
        ("finish", 1, 2),
        ("finish", 1, 3),
        ("finish", 1, 1),
        ("finish", 0, 3),
        ("finish", 0, 2),
    ),
    (
        ("near", 0),
        ("spread", 3, 1),
        ("spread", 2, 1),
        ("pass_on", 0, 2),
        ("pass_on", 0, 0),
        ("pass_on", 0, 3),
        ("pass_on", 0, 1),
        ("spread", 3, 0),
        ("spread", 2, 2),
        ("spread", 2, 3),
        ("spread", 2, 0),
        ("far", 0),
        ("pass_on", 2, 1),
        ("pass_on", 2, 3),
        ("spread", 1, 1),
        ("pass_on", 2, 2),
        ("pass_on", 3, 1),
        ("pass_on", 3, 0),
        ("pass_on", 2, 0),
        ("spread", 1, 3),
        ("spread", 3, 3),
        ("far", 2),
        ("spread", 3, 2),
        ("give", 2, 1),
        ("give", 2, 0),
        ("give", 2, 3),
        ("give", 2, 2),
        ("near", 2),
        ("pass_on", 1, 1),
        ("finish", 2, 1),
        ("spread", 1, 0),
        ("finish", 2, 0),
        ("pass_on", 3, 3),
        ("spread", 1, 2),
        ("pass_on", 3, 2),
        ("finish", 2, 3),
        ("far", 3),
        ("give", 0, 1),
        ("finish", 2, 2),
        ("pass_on", 1, 0),
        ("give", 3, 2),
        ("give", 0, 0),
        ("give", 3, 1),
        ("give", 3, 3),
        ("give", 3, 0),
        ("pass_on", 1, 2),
        ("pass_on", 1, 3),
        ("near", 3),
        ("far", 1),
        ("give", 1, 0),
        ("near", 1),
        ("finish", 3, 2),
        ("finish", 0, 1),
        ("give", 1, 3),
        ("give", 1, 2),
        ("finish", 3, 0),
        ("give", 1, 1),
        ("finish", 0, 0),
        ("finish", 3, 3),
        ("give", 0, 3),
        ("finish", 1, 0),
        ("finish", 1, 3),
        ("finish", 3, 1),
        ("finish", 1, 2),
        ("give", 0, 2),
        ("finish", 1, 1),
        ("finish", 0, 3),
        ("finish", 0, 2),
    ),
)


def mix_index(first, second, count):
    total = first * 0
    bit = 1
    while bit < count:
        one, two = (first // bit) % 2, (second // bit) % 2
        total = total + bit * (one + two - 2 * one * two)
        bit *= 2
    return total


def mark(order):
    seen, steps = set(), []
    for step in order:
        if step[0] == "finish":
            step = step + (step[1] not in seen,)
            seen.add(step[1])
        steps.append(step)
    return steps


def segments(order):
    parts = [[]]
    for step in mark(order)[:-1]:
        if step[0] in ("far", "near"):
            parts += [[step], []]
        else:
            parts[-1].append(step)
    return parts


def kernel(
    experts, cap,
    tok_hbm, gain_hbm, ids_hbm, weight_hbm, gate_ref, up_ref, down_ref,
    out_ref,
    tok_ref, gain_ref, ids_ref, weight_ref, norm, names, ranks, sides, picks, xs, xa, hid, po, rd, cx, rx, fo, ret, wgu, wd,
    in_sem, wgu_sem, wd_sem,
    z_send, z_recv, x_send, x_recv, d_send, d_recv, e_send, e_recv,
    r_send, r_recv, n_recv, v_send, v_recv, w_send, w_recv,
):
    ep, c = lax.axis_index("ep"), lax.axis_index("tp")
    p, h = ep // 2, ep % 2
    toks, width = tok_ref.shape
    tiles = wgu.shape[0]
    part_width = width // PIECES
    across = {"ep": 2 * p + 1 - h, "tp": c}
    beside = {"ep": ep, "tp": 1 - c}

    def plane(q):
        return {"ep": 2 * q + h, "tp": c}

    loads = [
        pltpu.make_async_copy(src, dst, in_sem.at[n]) for n, (src, dst) in enumerate((
            (tok_hbm, tok_ref), (gain_hbm, gain_ref), (ids_hbm, ids_ref), (weight_hbm, weight_ref)))]
    for load in loads:
        load.start()

    barrier = pltpu.get_barrier_semaphore()

    def greet(k, carry):
        pl.semaphore_signal(barrier, inc=1, device_id=plane(mix_index(p, k, experts)), device_id_type=MESH)
        return carry

    lax.fori_loop(1, experts, greet, 0)
    pl.semaphore_signal(barrier, inc=1, device_id=across, device_id_type=MESH)
    pl.semaphore_signal(barrier, inc=1, device_id=beside, device_id_type=MESH)

    def gate_copy(j):
        return pltpu.make_async_copy(
            gate_ref.at[:, pl.ds(j * LANE, LANE)], wgu.at[j, :, pl.ds(0, LANE)], wgu_sem)

    def up_copy(j):
        return pltpu.make_async_copy(
            up_ref.at[:, pl.ds(j * LANE, LANE)], wgu.at[j, :, pl.ds(LANE, LANE)], wgu_sem)

    down_copy = pltpu.make_async_copy(down_ref, wd, wd_sem)
    for j in range(tiles):
        gate_copy(j).start()
        up_copy(j).start()
    down_copy.start()

    row = lax.broadcasted_iota(jnp.int32, (toks, toks), 0)
    col = lax.broadcasted_iota(jnp.int32, (toks, toks), 1)
    before = (row < col).astype(jnp.float32).astype(jnp.bfloat16)
    slots = lax.broadcasted_iota(jnp.int32, (cap, toks), 0).astype(jnp.float32)
    for load in loads[1:]:
        load.wait()
    kinds = lax.broadcasted_iota(jnp.int32, names.shape, 0)
    names[...] = ((ids_ref[0:1, :] == kinds) | (ids_ref[1:2, :] == kinds)).astype(jnp.float32)
    ranks[...] = jnp.dot(names[...].astype(jnp.bfloat16), before, preferred_element_type=jnp.float32)

    loads[0].wait()
    values = tok_ref[...].astype(jnp.float32)
    scale_rows = lax.rsqrt(jnp.mean(values * values, axis=1, keepdims=True) + 1e-06)
    norm[...] = (values * scale_rows * gain_ref[...]).astype(jnp.bfloat16)

    def remote(src, dst, send, recv, target):
        return pltpu.make_async_remote_copy(
            src_ref=src, dst_ref=dst, send_sem=send, recv_sem=recv, device_id=target, device_id_type=MESH)

    def cut(ref, index, g):
        return ref.at[index, :, pl.ds(g * part_width, part_width)]

    def z_pair(k, g, origin):
        q = mix_index(p, k, experts)
        n = PIECES * (k - 1) + g
        return remote(
            cut(xs, q, g), cut(xa, 4 * origin(q) + 2 * h + c, g), z_send, z_recv.at[n], plane(q))

    def z_copy(k, g):
        return z_pair(k, g, lambda q: p)

    def z_land(k, g):
        return z_pair(k, g, lambda q: q)

    def mine(k, half, core, g):
        return cut(xa, 4 * mix_index(p, k, experts) + 2 * half + core, g)

    def x_copy(k, g):
        return remote(mine(k, h, c, g), mine(k, h, c, g), x_send, x_recv.at[PIECES * k + g], across)

    def x_land(k, g):
        return remote(mine(k, h, c, g), mine(k, 1 - h, c, g), x_send, x_recv.at[PIECES * k + g], across)

    def d_copy(k, g):
        return remote(mine(k, h, c, g), mine(k, h, c, g), d_send, d_recv.at[k], beside)

    def e_copy(k, g):
        return remote(mine(k, 1 - h, c, g), mine(k, 1 - h, c, g), e_send, e_recv.at[k], beside)

    def landing(k, half, send, recv):
        first = 4 * mix_index(p, k, experts) + 2 * half
        return remote(xa.at[first + c], xa.at[first + 1 - c], send, recv.at[k], beside)

    def r_copy(k, g, own):
        half = h if own else 1 - h
        recv = n_recv.at[k] if own else r_recv.at[PIECES * k + g]
        return remote(cut(po, 4 * k + 2 * half + 1 - c, g), cut(rd, 2 * k + half, g), r_send, recv, beside)

    def n_land(k):
        return remote(po.at[4 * k + 2 * h + 1 - c], rd.at[2 * k + h], r_send, n_recv.at[k], beside)

    def v_copy(k, g):
        n = PIECES * k + g
        return remote(cut(cx, k, g), cut(rx, k, g), v_send, v_recv.at[n], across)

    def w_copy(k, g):
        q = mix_index(p, k, experts)
        return remote(cut(fo, k, g), cut(ret, p, g), w_send, w_recv.at[g], plane(q))

    def w_land(g):
        cols = pl.ds(g * part_width, part_width)
        return remote(
            fo.at[pl.ds(0, experts - 1), :, cols], ret.at[pl.ds(0, experts - 1), :, cols],
            w_send, w_recv.at[g], beside)

    def picked(e):
        spot = pl.ds(e, 1)
        pick = jnp.where(slots == ranks[spot, :], names[spot, :], 0.0).astype(jnp.bfloat16)
        return jnp.dot(pick, norm[...], preferred_element_type=jnp.float32).astype(jnp.bfloat16)

    inner = (p + 1) // 2 % 2

    def turn(s):
        outside, inside = TURNS[0][s], TURNS[1][s]
        return outside if outside == inside else outside + inner * (inside - outside)

    pl.semaphore_wait(barrier, experts + 1)

    xa[4 * p + 2 * h + c] = picked(p)
    for g in range(PIECES):
        x_copy(0, g).start()
        d_copy(0, g).start()

    if experts == len(TURNS[0]):
        for k in range(1, experts):
            xs[mix_index(p, k, experts)] = picked(mix_index(p, k, experts))
        for side, sends in enumerate(SENDS):
            @pl.when(inner == side)
            def _():
                for s, g in sends:
                    z_copy(TURNS[side][s], g).start()
    else:
        def fill(k, carry):
            e = mix_index(p, k, experts)
            xs[e] = picked(e)
            for g in range(PIECES):
                z_copy(k, g).start()
            return carry

        lax.fori_loop(1, experts, fill, 0)

    step = 2 * LANE

    def compute(k, own):
        half = h if own else 1 - h
        rows = xa[pl.ds(4 * mix_index(p, k, experts) + 2 * half, 2)].reshape(2 * cap, width)
        for j in range(tiles):
            both = jnp.dot(rows, wgu[j], preferred_element_type=jnp.float32)
            gate, up = both[:, :LANE], both[:, LANE:]
            hid[:, j * LANE:(j + 1) * LANE] = (gate / (1.0 + jnp.exp(-gate)) * up).astype(jnp.bfloat16)
        many = part_width // step
        for g in range(PIECES):
            for n in range(g * many, (g + 1) * many):
                part = jnp.dot(hid[...], wd[:, n * step:(n + 1) * step], preferred_element_type=jnp.float32)
                po[pl.ds(4 * k + 2 * half, 2), :, n * step:(n + 1) * step] = part.astype(
                    jnp.bfloat16).reshape(2, cap, step)
            r_copy(k, g, own).start()

    def add(first, second):
        return (first.astype(jnp.float32) + second.astype(jnp.float32)).astype(jnp.bfloat16)

    def spread(k, g):
        z_land(k, g).wait_recv()
        x_copy(k, g).start()
        d_copy(k, g).start()

    def pass_on(k, g):
        x_land(k, g).wait_recv()
        e_copy(k, g).start()

    def far(k):
        landing(k, 1 - h, e_send, e_recv).wait_recv()
        compute(k, False)

    def near(k):
        landing(k, h, d_send, d_recv).wait_recv()
        compute(k, True)

    def joined(k, half, g):
        cols = pl.ds(g * part_width, part_width)
        return add(po[4 * k + 2 * half + c, :, cols], rd[2 * k + half, :, cols])

    def give(k, g):
        r_copy(k, g, False).wait_recv()
        cx[k, :, g * part_width:(g + 1) * part_width] = joined(k, 1 - h, g)
        v_copy(k, g).start()

    def finish(k, g, first):
        cols = pl.ds(g * part_width, part_width)
        if first:
            n_land(k).wait_recv()
        here = joined(k, h, g)
        v_copy(k, g).wait_recv()
        total = add(here, rx[k, :, cols])
        if isinstance(k, int) and k == 0:
            ret[p, :, cols] = total
        else:
            fo[k, :, cols] = total
            w_copy(k, g).start()

    after = (col < row).astype(jnp.float32).astype(jnp.bfloat16)

    sides[...] = jnp.concatenate(
        [ids_ref[...].astype(jnp.float32), weight_ref[...], jnp.zeros((LANE - 4, toks), jnp.float32)], axis=0).T

    def place_of(e, places):
        number = lax.convert_element_type(e, jnp.float32)
        hits = [(sides[:, n:n + 1] == number).astype(jnp.float32) for n in range(2)]
        rank = jnp.dot(
            after, jnp.broadcast_to(hits[0] + hits[1], (toks, LANE)).astype(jnp.bfloat16),
            preferred_element_type=jnp.float32)[:, 0:1]
        spot = rank + number * cap
        return tuple(old + hit * spot for old, hit in zip(places, hits))

    zero = jnp.zeros((toks, 1), jnp.float32)
    places = lax.fori_loop(0, experts, place_of, (zero, zero))
    lanes = lax.broadcasted_iota(jnp.int32, (toks, experts * cap), 1).astype(jnp.float32)
    for m in range(2):
        picks[m] = (lanes == places[m]).astype(jnp.float32).astype(jnp.bfloat16)

    pltpu.make_async_copy(wgu, wgu, wgu_sem).wait()
    down_copy.wait()

    def sent(ref, count, send, recv):
        part = ref.at[pl.ds(0, count)]
        remote(part, part, send, recv.at[0], beside).wait_send()

    def settle():
        sent(xs, experts - 1, z_send, z_recv)
        sent(xa, experts, x_send, x_recv)
        sent(xa, experts, d_send, d_recv)
        sent(xa, experts, e_send, e_recv)
        sent(po, 2 * experts, r_send, r_recv)

    events = dict(spread=spread, pass_on=pass_on, far=far, near=near, give=give, finish=finish)
    if experts == len(TURNS[0]):
        def run(steps, place):
            for name, s, *rest in steps:
                events[name](place(s), *rest)

        for n, (outside, inside) in enumerate(zip(*map(segments, ORDERS))):
            if outside == inside:
                run(outside, turn)
            else:
                for side, steps in enumerate((outside, inside)):
                    @pl.when(inner == side)
                    def _():
                        run(steps, lambda s: TURNS[side][s])
        settle()
        run([mark(ORDERS[0])[-1]], turn)
    else:
        def each(event, k):
            for g in range(PIECES):
                event(k, g, *([g == 0] if event is finish else []))

        def stage(k, carry):
            near(k)

            @pl.when(k + 1 < experts)
            def _():
                each(spread, k + 1)

            each(pass_on, k)
            far(k)

            @pl.when(k > 1)
            def _():
                each(finish, k - 1)

            @pl.when(k > 0)
            def _():
                each(give, k)

            return carry

        lax.fori_loop(0, experts, stage, 0)
        each(give, 0)
        each(finish, experts - 1)
        settle()
        each(finish, 0)

    for g in range(PIECES):
        w_land(g).wait_recv()
        cols = pl.ds(g * part_width, part_width)
        rows = ret[:, :, cols].reshape(experts * cap, part_width)
        total = jnp.zeros((toks, part_width), jnp.float32)
        for m in range(2):
            total = total + sides[:, 2 + m:3 + m] * jnp.dot(
                picks[m], rows, preferred_element_type=jnp.float32)
        out_ref[:, cols] = total.astype(jnp.bfloat16)
    sent(cx, experts, v_send, v_recv)
    sent(fo, experts - 1, w_send, w_recv)


def local(tokens, norm_gain, expert_ids, route_weights, w_gate, w_up, w_down):
    experts = lax.axis_size("ep") // 2
    toks, width = tokens.shape
    hidden = w_gate.shape[1]
    capacity = 2 * max(1, 5 * toks * expert_ids.shape[1] // (8 * experts))
    cap = -(-capacity // 16) * 16
    tiles = hidden // LANE
    kinds = -(-experts // 16) * 16
    any_space = pl.BlockSpec(memory_space=pl.ANY)
    dma = pltpu.SemaphoreType.DMA
    bf16 = jnp.bfloat16
    return pl.pallas_call(
        functools.partial(kernel, experts, cap),
        out_shape=pltpu.VMEM((toks, width), bf16),
        in_specs=[any_space] * 7,
        out_specs=pl.BlockSpec(memory_space=pltpu.VMEM),
        scratch_shapes=[
            pltpu.VMEM((toks, width), bf16),
            pltpu.VMEM((1, width), jnp.float32),
            pltpu.VMEM((2, toks), jnp.int32),
            pltpu.VMEM((2, toks), jnp.float32),
            pltpu.VMEM((toks, width), bf16),
            pltpu.VMEM((kinds, toks), jnp.float32),
            pltpu.VMEM((kinds, toks), jnp.float32),
            pltpu.VMEM((toks, LANE), jnp.float32),
            pltpu.VMEM((2, toks, experts * cap), bf16),
            pltpu.VMEM((experts, cap, width), bf16),
            pltpu.VMEM((experts * 4, cap, width), bf16),
            pltpu.VMEM((2 * cap, hidden), bf16),
            pltpu.VMEM((experts * 4, cap, width), bf16),
            pltpu.VMEM((experts * 2, cap, width), bf16),
            pltpu.VMEM((experts, cap, width), bf16),
            pltpu.VMEM((experts, cap, width), bf16),
            pltpu.VMEM((experts, cap, width), bf16),
            pltpu.VMEM((experts, cap, width), bf16),
            pltpu.VMEM((tiles, width, 2 * LANE), bf16),
            pltpu.VMEM((hidden, width), bf16),
            dma((4,)), dma, dma,
            dma, dma((PIECES * (experts - 1),)), dma, dma((PIECES * experts,)),
            dma, dma((experts,)), dma, dma((experts,)),
            dma, dma((PIECES * experts,)), dma((experts,)), dma, dma((PIECES * experts,)), dma, dma((PIECES,)),
        ],
        compiler_params=pltpu.CompilerParams(
            collective_id=0, has_side_effects=True, vmem_limit_bytes=60 * 1024 * 1024),
    )(tokens, norm_gain.reshape(1, -1), expert_ids.T, route_weights.T, w_gate, w_up, w_down)


def solution(mesh):
    placed = (
        P(("grp", "ep", "tp"), None),
        P(),
        P(("grp", "ep", "tp"), None),
        P(("grp", "ep", "tp"), None),
        P(None, ("ep", "tp")),
        P(None, ("ep", "tp")),
        P(("ep", "tp"), None),
    )
    return jax.shard_map(
        local, mesh=mesh, in_specs=placed, out_specs=P(("grp", "ep", "tp"), None), check_vma=False
    )
```

```python
import functools

import jax
import jax.numpy as jnp
from jax import lax
from jax.experimental import pallas as pl
from jax.experimental.pallas import tpu as pltpu
from jax.sharding import PartitionSpec as P

MESH = pl.DeviceIdType.MESH
LANE = 128
PIECES = 4
TURNS = ((0, 1, 3, 2), (0, 3, 2, 1))
SENDS = (
    (
        (2, 3),
        (1, 1),
        (3, 1),
        (1, 0),
        (3, 2),
        (3, 3),
        (3, 0),
        (2, 2),
        (2, 0),
        (2, 1),
        (1, 3),
        (1, 2),
    ),
    (
        (2, 2),
        (3, 1),
        (1, 1),
        (3, 3),
        (1, 3),
        (2, 0),
        (3, 2),
        (2, 1),
        (2, 3),
        (3, 0),
        (1, 0),
        (1, 2),
    ),
)
ORDERS = (
    (
        ("near", 0),
        ("pass_on", 0, 0),
        ("spread", 1, 1),
        ("spread", 2, 3),
        ("pass_on", 0, 3),
        ("spread", 3, 2),
        ("pass_on", 0, 1),
        ("pass_on", 0, 2),
        ("spread", 1, 0),
        ("spread", 1, 2),
        ("spread", 1, 3),
        ("far", 0),
        ("spread", 2, 2),
        ("spread", 2, 0),
        ("spread", 2, 1),
        ("pass_on", 2, 2),
        ("give", 0, 1),
        ("spread", 3, 0),
        ("pass_on", 1, 1),
        ("pass_on", 2, 3),
        ("pass_on", 2, 1),
        ("pass_on", 2, 0),
        ("spread", 3, 1),
        ("spread", 3, 3),
        ("far", 2),
        ("give", 2, 0),
        ("pass_on", 1, 0),
        ("give", 0, 0),
        ("pass_on", 3, 0),
        ("pass_on", 1, 2),
        ("pass_on", 3, 1),
        ("pass_on", 3, 2),
        ("pass_on", 1, 3),
        ("give", 2, 1),
        ("near", 2),
        ("pass_on", 3, 3),
        ("give", 2, 2),
        ("give", 2, 3),
        ("finish", 2, 0),
        ("far", 3),
        ("finish", 2, 1),
        ("give", 3, 0),
        ("near", 3),
        ("finish", 2, 2),
        ("give", 3, 2),
        ("give", 3, 3),
        ("finish", 0, 1),
        ("finish", 2, 3),
        ("far", 1),
        ("finish", 3, 0),
        ("give", 3, 1),
        ("give", 1, 0),
        ("give", 1, 2),
        ("give", 1, 3),
        ("finish", 3, 2),
        ("give", 1, 1),
        ("give", 0, 3),
        ("finish", 0, 0),
        ("finish", 3, 3),
        ("near", 1),
        ("give", 0, 2),
        ("finish", 3, 1),
        ("finish", 1, 0),
        ("finish", 1, 2),
        ("finish", 1, 3),
        ("finish", 1, 1),
        ("finish", 0, 3),
        ("finish", 0, 2),
    ),
    (
        ("near", 0),
        ("spread", 3, 1),
        ("spread", 2, 1),
        ("pass_on", 0, 2),
        ("pass_on", 0, 0),
        ("pass_on", 0, 3),
        ("pass_on", 0, 1),
        ("spread", 3, 0),
        ("spread", 2, 2),
        ("spread", 2, 3),
        ("spread", 2, 0),
        ("far", 0),
        ("pass_on", 2, 1),
        ("pass_on", 2, 3),
        ("spread", 1, 1),
        ("pass_on", 2, 2),
        ("pass_on", 3, 1),
        ("pass_on", 3, 0),
        ("pass_on", 2, 0),
        ("spread", 1, 3),
        ("spread", 3, 3),
        ("far", 2),
        ("spread", 3, 2),
        ("give", 2, 1),
        ("give", 2, 0),
        ("give", 2, 3),
        ("give", 2, 2),
        ("near", 2),
        ("pass_on", 1, 1),
        ("finish", 2, 1),
        ("spread", 1, 0),
        ("finish", 2, 0),
        ("pass_on", 3, 3),
        ("spread", 1, 2),
        ("pass_on", 3, 2),
        ("finish", 2, 3),
        ("far", 3),
        ("give", 0, 1),
        ("finish", 2, 2),
        ("pass_on", 1, 0),
        ("give", 3, 2),
        ("give", 0, 0),
        ("give", 3, 1),
        ("give", 3, 3),
        ("give", 3, 0),
        ("pass_on", 1, 2),
        ("pass_on", 1, 3),
        ("near", 3),
        ("far", 1),
        ("give", 1, 0),
        ("near", 1),
        ("finish", 3, 2),
        ("finish", 0, 1),
        ("give", 1, 3),
        ("give", 1, 2),
        ("finish", 3, 0),
        ("give", 1, 1),
        ("finish", 0, 0),
        ("finish", 3, 3),
        ("give", 0, 3),
        ("finish", 1, 0),
        ("finish", 1, 3),
        ("finish", 3, 1),
        ("finish", 1, 2),
        ("give", 0, 2),
        ("finish", 1, 1),
        ("finish", 0, 3),
        ("finish", 0, 2),
    ),
)


def mix_index(first, second, count):
    total = first * 0
    bit = 1
    while bit < count:
        one, two = (first // bit) % 2, (second // bit) % 2
        total = total + bit * (one + two - 2 * one * two)
        bit *= 2
    return total


def mark(order):
    seen, steps = set(), []
    for step in order:
        if step[0] == "finish":
            step = step + (step[1] not in seen,)
            seen.add(step[1])
        steps.append(step)
    return steps


def segments(order):
    parts = [[]]
    for step in mark(order)[:-1]:
        if step[0] in ("far", "near"):
            parts += [[step], []]
        else:
            parts[-1].append(step)
    return parts


def kernel(
    experts, cap,
    tok_hbm, gain_hbm, ids_hbm, weight_hbm, gate_ref, up_ref, down_ref,
    out_ref,
    tok_ref, gain_ref, ids_ref, weight_ref, norm, names, ranks, sides, picks, xs, xa, hid, po, rd, cx, rx, fo, ret, wgu, wd,
    in_sem, wgu_sem, wd_sem,
    z_send, z_recv, x_send, x_recv, d_send, d_recv, e_send, e_recv,
    r_send, r_recv, n_recv, v_send, v_recv, w_send, w_recv,
):
    ep, c = lax.axis_index("ep"), lax.axis_index("tp")
    p, h = ep // 2, ep % 2
    toks, width = tok_ref.shape
    tiles = wgu.shape[0]
    part_width = width // PIECES
    across = {"ep": 2 * p + 1 - h, "tp": c}
    beside = {"ep": ep, "tp": 1 - c}

    def plane(q):
        return {"ep": 2 * q + h, "tp": c}

    loads = [
        pltpu.make_async_copy(src, dst, in_sem.at[n]) for n, (src, dst) in enumerate((
            (tok_hbm, tok_ref), (gain_hbm, gain_ref), (ids_hbm, ids_ref), (weight_hbm, weight_ref)))]
    for load in loads:
        load.start()

    barrier = pltpu.get_barrier_semaphore()

    def greet(k, carry):
        pl.semaphore_signal(barrier, inc=1, device_id=plane(mix_index(p, k, experts)), device_id_type=MESH)
        return carry

    lax.fori_loop(1, experts, greet, 0)
    pl.semaphore_signal(barrier, inc=1, device_id=across, device_id_type=MESH)
    pl.semaphore_signal(barrier, inc=1, device_id=beside, device_id_type=MESH)

    def gate_copy(j):
        return pltpu.make_async_copy(
            gate_ref.at[:, pl.ds(j * LANE, LANE)], wgu.at[j, :, pl.ds(0, LANE)], wgu_sem)

    def up_copy(j):
        return pltpu.make_async_copy(
            up_ref.at[:, pl.ds(j * LANE, LANE)], wgu.at[j, :, pl.ds(LANE, LANE)], wgu_sem)

    down_copy = pltpu.make_async_copy(down_ref, wd, wd_sem)
    for j in range(tiles):
        gate_copy(j).start()
        up_copy(j).start()
    down_copy.start()

    row = lax.broadcasted_iota(jnp.int32, (toks, toks), 0)
    col = lax.broadcasted_iota(jnp.int32, (toks, toks), 1)
    before = (row < col).astype(jnp.float32).astype(jnp.bfloat16)
    slots = lax.broadcasted_iota(jnp.int32, (cap, toks), 0).astype(jnp.float32)
    for load in loads[1:]:
        load.wait()
    kinds = lax.broadcasted_iota(jnp.int32, names.shape, 0)
    names[...] = ((ids_ref[0:1, :] == kinds) | (ids_ref[1:2, :] == kinds)).astype(jnp.float32)
    ranks[...] = jnp.dot(names[...].astype(jnp.bfloat16), before, preferred_element_type=jnp.float32)

    loads[0].wait()
    values = tok_ref[...].astype(jnp.float32)
    scale_rows = lax.rsqrt(jnp.mean(values * values, axis=1, keepdims=True) + 1e-06)
    norm[...] = (values * scale_rows * gain_ref[...]).astype(jnp.bfloat16)

    def remote(src, dst, send, recv, target):
        return pltpu.make_async_remote_copy(
            src_ref=src, dst_ref=dst, send_sem=send, recv_sem=recv, device_id=target, device_id_type=MESH)

    def cut(ref, index, g):
        return ref.at[index, :, pl.ds(g * part_width, part_width)]

    def z_pair(k, g, origin):
        q = mix_index(p, k, experts)
        n = PIECES * (k - 1) + g
        return remote(
            cut(xs, q, g), cut(xa, 4 * origin(q) + 2 * h + c, g), z_send, z_recv.at[n], plane(q))

    def z_copy(k, g):
        return z_pair(k, g, lambda q: p)

    def z_land(k, g):
        return z_pair(k, g, lambda q: q)

    def mine(k, half, core, g):
        return cut(xa, 4 * mix_index(p, k, experts) + 2 * half + core, g)

    def x_copy(k, g):
        return remote(mine(k, h, c, g), mine(k, h, c, g), x_send, x_recv.at[PIECES * k + g], across)

    def x_land(k, g):
        return remote(mine(k, h, c, g), mine(k, 1 - h, c, g), x_send, x_recv.at[PIECES * k + g], across)

    def d_copy(k, g):
        return remote(mine(k, h, c, g), mine(k, h, c, g), d_send, d_recv.at[k], beside)

    def e_copy(k, g):
        return remote(mine(k, 1 - h, c, g), mine(k, 1 - h, c, g), e_send, e_recv.at[k], beside)

    def landing(k, half, send, recv):
        first = 4 * mix_index(p, k, experts) + 2 * half
        return remote(xa.at[first + c], xa.at[first + 1 - c], send, recv.at[k], beside)

    def r_copy(k, g, own):
        half = h if own else 1 - h
        recv = n_recv.at[k] if own else r_recv.at[PIECES * k + g]
        return remote(cut(po, 4 * k + 2 * half + 1 - c, g), cut(rd, 2 * k + half, g), r_send, recv, beside)

    def n_land(k):
        return remote(po.at[4 * k + 2 * h + 1 - c], rd.at[2 * k + h], r_send, n_recv.at[k], beside)

    def v_copy(k, g):
        n = PIECES * k + g
        return remote(cut(cx, k, g), cut(rx, k, g), v_send, v_recv.at[n], across)

    def w_copy(k, g):
        q = mix_index(p, k, experts)
        return remote(cut(fo, k, g), cut(ret, p, g), w_send, w_recv.at[g], plane(q))

    def w_land(g):
        cols = pl.ds(g * part_width, part_width)
        return remote(
            fo.at[pl.ds(0, experts - 1), :, cols], ret.at[pl.ds(0, experts - 1), :, cols],
            w_send, w_recv.at[g], beside)

    def picked(e):
        spot = pl.ds(e, 1)
        pick = jnp.where(slots == ranks[spot, :], names[spot, :], 0.0).astype(jnp.bfloat16)
        return jnp.dot(pick, norm[...], preferred_element_type=jnp.float32).astype(jnp.bfloat16)

    inner = (p + 1) // 2 % 2

    def turn(s):
        outside, inside = TURNS[0][s], TURNS[1][s]
        return outside if outside == inside else outside + inner * (inside - outside)

    xa[4 * p + 2 * h + c] = picked(p)
    if experts == len(TURNS[0]):
        for k in range(1, experts):
            xs[mix_index(p, k, experts)] = picked(mix_index(p, k, experts))

    pl.semaphore_wait(barrier, experts + 1)

    for g in range(PIECES):
        x_copy(0, g).start()
        d_copy(0, g).start()

    if experts == len(TURNS[0]):
        for side, sends in enumerate(SENDS):
            @pl.when(inner == side)
            def _():
                for s, g in sends:
                    z_copy(TURNS[side][s], g).start()
    else:
        def fill(k, carry):
            e = mix_index(p, k, experts)
            xs[e] = picked(e)
            for g in range(PIECES):
                z_copy(k, g).start()
            return carry

        lax.fori_loop(1, experts, fill, 0)

    step = 2 * LANE

    def compute(k, own):
        half = h if own else 1 - h
        rows = xa[pl.ds(4 * mix_index(p, k, experts) + 2 * half, 2)].reshape(2 * cap, width)
        for j in range(tiles):
            both = jnp.dot(rows, wgu[j], preferred_element_type=jnp.float32)
            gate, up = both[:, :LANE], both[:, LANE:]
            hid[:, j * LANE:(j + 1) * LANE] = (gate / (1.0 + jnp.exp(-gate)) * up).astype(jnp.bfloat16)
        many = part_width // step
        for g in range(PIECES):
            for n in range(g * many, (g + 1) * many):
                part = jnp.dot(hid[...], wd[:, n * step:(n + 1) * step], preferred_element_type=jnp.float32)
                po[pl.ds(4 * k + 2 * half, 2), :, n * step:(n + 1) * step] = part.astype(
                    jnp.bfloat16).reshape(2, cap, step)
            r_copy(k, g, own).start()

    def add(first, second):
        return (first.astype(jnp.float32) + second.astype(jnp.float32)).astype(jnp.bfloat16)

    def spread(k, g):
        z_land(k, g).wait_recv()
        x_copy(k, g).start()
        d_copy(k, g).start()

    def pass_on(k, g):
        x_land(k, g).wait_recv()
        e_copy(k, g).start()

    def far(k):
        landing(k, 1 - h, e_send, e_recv).wait_recv()
        compute(k, False)

    def near(k):
        landing(k, h, d_send, d_recv).wait_recv()
        compute(k, True)

    def joined(k, half, g):
        cols = pl.ds(g * part_width, part_width)
        return add(po[4 * k + 2 * half + c, :, cols], rd[2 * k + half, :, cols])

    def give(k, g):
        r_copy(k, g, False).wait_recv()
        cx[k, :, g * part_width:(g + 1) * part_width] = joined(k, 1 - h, g)
        v_copy(k, g).start()

    def finish(k, g, first):
        cols = pl.ds(g * part_width, part_width)
        if first:
            n_land(k).wait_recv()
        here = joined(k, h, g)
        v_copy(k, g).wait_recv()
        total = add(here, rx[k, :, cols])
        if isinstance(k, int) and k == 0:
            ret[p, :, cols] = total
        else:
            fo[k, :, cols] = total
            w_copy(k, g).start()

    after = (col < row).astype(jnp.float32).astype(jnp.bfloat16)

    sides[...] = jnp.concatenate(
        [ids_ref[...].astype(jnp.float32), weight_ref[...], jnp.zeros((LANE - 4, toks), jnp.float32)], axis=0).T

    def place_of(e, places):
        number = lax.convert_element_type(e, jnp.float32)
        hits = [(sides[:, n:n + 1] == number).astype(jnp.float32) for n in range(2)]
        rank = jnp.dot(
            after, jnp.broadcast_to(hits[0] + hits[1], (toks, LANE)).astype(jnp.bfloat16),
            preferred_element_type=jnp.float32)[:, 0:1]
        spot = rank + number * cap
        return tuple(old + hit * spot for old, hit in zip(places, hits))

    zero = jnp.zeros((toks, 1), jnp.float32)
    places = lax.fori_loop(0, experts, place_of, (zero, zero))
    lanes = lax.broadcasted_iota(jnp.int32, (toks, experts * cap), 1).astype(jnp.float32)
    for m in range(2):
        picks[m] = (lanes == places[m]).astype(jnp.float32).astype(jnp.bfloat16)

    pltpu.make_async_copy(wgu, wgu, wgu_sem).wait()
    down_copy.wait()

    def sent(ref, count, send, recv):
        part = ref.at[pl.ds(0, count)]
        remote(part, part, send, recv.at[0], beside).wait_send()

    def settle():
        sent(xs, experts - 1, z_send, z_recv)
        sent(xa, experts, x_send, x_recv)
        sent(xa, experts, d_send, d_recv)
        sent(xa, experts, e_send, e_recv)
        sent(po, 2 * experts, r_send, r_recv)

    events = dict(spread=spread, pass_on=pass_on, far=far, near=near, give=give, finish=finish)
    if experts == len(TURNS[0]):
        def run(steps, place):
            for name, s, *rest in steps:
                events[name](place(s), *rest)

        for n, (outside, inside) in enumerate(zip(*map(segments, ORDERS))):
            if outside == inside:
                run(outside, turn)
            else:
                for side, steps in enumerate((outside, inside)):
                    @pl.when(inner == side)
                    def _():
                        run(steps, lambda s: TURNS[side][s])
        settle()
        run([mark(ORDERS[0])[-1]], turn)
    else:
        def each(event, k):
            for g in range(PIECES):
                event(k, g, *([g == 0] if event is finish else []))

        def stage(k, carry):
            near(k)

            @pl.when(k + 1 < experts)
            def _():
                each(spread, k + 1)

            each(pass_on, k)
            far(k)

            @pl.when(k > 1)
            def _():
                each(finish, k - 1)

            @pl.when(k > 0)
            def _():
                each(give, k)

            return carry

        lax.fori_loop(0, experts, stage, 0)
        each(give, 0)
        each(finish, experts - 1)
        settle()
        each(finish, 0)

    for g in range(PIECES):
        w_land(g).wait_recv()
        cols = pl.ds(g * part_width, part_width)
        rows = ret[:, :, cols].reshape(experts * cap, part_width)
        total = jnp.zeros((toks, part_width), jnp.float32)
        for m in range(2):
            total = total + sides[:, 2 + m:3 + m] * jnp.dot(
                picks[m], rows, preferred_element_type=jnp.float32)
        out_ref[:, cols] = total.astype(jnp.bfloat16)
    sent(cx, experts, v_send, v_recv)
    sent(fo, experts - 1, w_send, w_recv)


def local(tokens, norm_gain, expert_ids, route_weights, w_gate, w_up, w_down):
    experts = lax.axis_size("ep") // 2
    toks, width = tokens.shape
    hidden = w_gate.shape[1]
    capacity = 2 * max(1, 5 * toks * expert_ids.shape[1] // (8 * experts))
    cap = -(-capacity // 16) * 16
    tiles = hidden // LANE
    kinds = -(-experts // 16) * 16
    any_space = pl.BlockSpec(memory_space=pl.ANY)
    dma = pltpu.SemaphoreType.DMA
    bf16 = jnp.bfloat16
    return pl.pallas_call(
        functools.partial(kernel, experts, cap),
        out_shape=pltpu.VMEM((toks, width), bf16),
        in_specs=[any_space] * 7,
        out_specs=pl.BlockSpec(memory_space=pltpu.VMEM),
        scratch_shapes=[
            pltpu.VMEM((toks, width), bf16),
            pltpu.VMEM((1, width), jnp.float32),
            pltpu.VMEM((2, toks), jnp.int32),
            pltpu.VMEM((2, toks), jnp.float32),
            pltpu.VMEM((toks, width), bf16),
            pltpu.VMEM((kinds, toks), jnp.float32),
            pltpu.VMEM((kinds, toks), jnp.float32),
            pltpu.VMEM((toks, LANE), jnp.float32),
            pltpu.VMEM((2, toks, experts * cap), bf16),
            pltpu.VMEM((experts, cap, width), bf16),
            pltpu.VMEM((experts * 4, cap, width), bf16),
            pltpu.VMEM((2 * cap, hidden), bf16),
            pltpu.VMEM((experts * 4, cap, width), bf16),
            pltpu.VMEM((experts * 2, cap, width), bf16),
            pltpu.VMEM((experts, cap, width), bf16),
            pltpu.VMEM((experts, cap, width), bf16),
            pltpu.VMEM((experts, cap, width), bf16),
            pltpu.VMEM((experts, cap, width), bf16),
            pltpu.VMEM((tiles, width, 2 * LANE), bf16),
            pltpu.VMEM((hidden, width), bf16),
            dma((4,)), dma, dma,
            dma, dma((PIECES * (experts - 1),)), dma, dma((PIECES * experts,)),
            dma, dma((experts,)), dma, dma((experts,)),
            dma, dma((PIECES * experts,)), dma((experts,)), dma, dma((PIECES * experts,)), dma, dma((PIECES,)),
        ],
        compiler_params=pltpu.CompilerParams(
            collective_id=0, has_side_effects=True, vmem_limit_bytes=60 * 1024 * 1024),
    )(tokens, norm_gain.reshape(1, -1), expert_ids.T, route_weights.T, w_gate, w_up, w_down)


def solution(mesh):
    placed = (
        P(("grp", "ep", "tp"), None),
        P(),
        P(("grp", "ep", "tp"), None),
        P(("grp", "ep", "tp"), None),
        P(None, ("ep", "tp")),
        P(None, ("ep", "tp")),
        P(("ep", "tp"), None),
    )
    return jax.shard_map(
        local, mesh=mesh, in_specs=placed, out_specs=P(("grp", "ep", "tp"), None), check_vma=False
    )
```
